512 devices in a mesh: ep: 128 (over z, y, core), tp: 4 (over x).
Axes of the slice: x: 4, y: 8, z: 8, core: 2. Of those that a mesh axis runs over, the one named last changes fastest.
Arguments:
- residual_in: bfloat16 [256, 2048], P('ep'), may hold values from -6 to 6
- gla_state: float32 [256, 4, 256, 512], P('ep', 'tp'), may hold values from -6 to 6
- norm_gain: bfloat16 [2048], replicated, may hold values from 0.099609375 to 1.8984375
- w_query: bfloat16 [2048, 1024], P('ep', 'tp'), may hold values from -0.125 to 0.125
- w_key: bfloat16 [2048, 1024], P('ep', 'tp'), may hold values from -0.125 to 0.125
- w_value: bfloat16 [2048, 2048], P('ep', 'tp'), may hold values from -0.125 to 0.125
- w_decay: bfloat16 [2048, 1024], P('ep', 'tp'), may hold values from -0.5 to 0.5
- decay_bias: float32 [1024], P('tp'), may hold values from -40 to 8
- head_gain: bfloat16 [512], replicated, may hold values from 0.099609375 to 1.8984375
- w_output: bfloat16 [2048, 2048], P('tp', 'ep'), may hold values from -0.125 to 0.125
- ffn_gain: bfloat16 [2048], replicated, may hold values from 0.099609375 to 1.8984375
- router_group: bfloat16 [2048, 4], replicated, may hold values from -0.125 to 0.125
- router_expert: bfloat16 [128, 2048], replicated, may hold values from -0.125 to 0.125
- expert_ids: int32 [256, 2], replicated, may hold values from 0 to 127, all different within a row; in each aligned block of 256 rows (0 to 255, 256 to 511, ...) at most 16 rows name the same one
- w_gate: bfloat16 [128, 2048, 512], P('ep', None, 'tp'), may hold values from -0.125 to 0.125
- w_up: bfloat16 [128, 2048, 512], P('ep', None, 'tp'), may hold values from -0.125 to 0.125
- w_down: bfloat16 [128, 512, 2048], P('ep', 'tp'), may hold values from -0.75 to 0.75
Outputs:
- layer_out: bfloat16 [256, 2048], P('ep')
- new_state: float32 [256, 4, 256, 512], P('ep', 'tp')
The draws below stay inside these ranges and needn't reach their ends.
Inputs may be any that keep to these rules, and one draw needn't show every extreme that they name: `expert_ids`: each row names 2 different experts; no expert is named by more than 16 rows of the whole batch, a bound that some block reaches.
All inputs are finite; a program needn't handle non-finite values.
Results may differ from the reference program's by a relative error of at most 0.023.
Values may be sent and summed in bfloat16 or wider, within the bound.
A program may use at most 64 MiB of HBM per device.

```python
import math
import jax
import jax.numpy as jnp
import numpy as np
from jax import lax

D = 2048
HEADS = 4
DKH = 256
DVH = 512
FF = 512
GROUPS = 4
TOP = 2
TOKENS = 256
EXPERTS = 128
CAP = 16
DK = 1024
DV = 2048


def draw_decay_bias(key, part):
    return jax.random.uniform(key, (HEADS * DKH,), jnp.float32, -40.0, 8.0)


def levels(own_key, shape, cuts, least, high):
    loudness = 1.0
    for axis_at, shards_of in cuts:
        heights = jax.random.uniform(jax.random.fold_in(jax.random.fold_in(own_key, 6), axis_at), (shards_of,), jnp.float32, least / len(cuts), high / len(cuts))
        loudness = loudness * jnp.repeat(jnp.exp(heights), shape[axis_at] // shards_of).reshape((-1,) + (1,) * (len(shape) - 1 - axis_at))
    return loudness


def deal_out(own_key, own, number, rows, count, top, reach, slope):
    sequence = jax.random.permutation(own_key, count)
    crowded, usual = portions_of(count, rows * top, reach, slope, True), portions_of(count, rows * top, reach, slope, False)
    places = jnp.arange(count)

    def named(lengths, rotation):
        used = int((lengths > 0).sum())
        fixed = max(1, used // 4)
        shifted = fixed + (places - fixed + rotation * (used - fixed)) % max(1, count - fixed)
        return jnp.zeros((count,), jnp.int32).at[sequence[jnp.where(places < fixed, places, shifted)]].set(jnp.asarray(lengths, jnp.int32))

    lengths = jnp.where(number % 4 == 0, named(crowded, number // 4), named(usual, number - number // 4 - 1))
    mixed = jax.random.permutation(jax.random.fold_in(own, 3), count)
    source_of, receiver = mixed[0:count // 2 * 2:2], mixed[1:count // 2 * 2:2]
    margin = jnp.minimum(lengths[source_of] - 1, reach - lengths[receiver]) // 2
    margin = jnp.where((source_of == sequence[0]) | (receiver == sequence[0]) | (lengths[receiver] == 0), 0, jnp.maximum(margin, 0))
    shifted = jax.random.randint(jax.random.fold_in(own, 4), (count // 2,), 0, 1 << 20) % (margin + 1)
    lengths = lengths.at[source_of].add(-shifted).at[receiver].add(shifted)
    labels = jnp.searchsorted(jnp.cumsum(lengths), jnp.arange(rows * top), side="right").astype(jnp.int32)
    listing = labels.reshape(top, rows).T
    listing = listing[jax.random.permutation(jax.random.fold_in(own, 1), rows)]
    rotation = jax.random.randint(jax.random.fold_in(own, 2), (rows, 1), 0, top)
    return jnp.take_along_axis(listing, (jnp.arange(top)[None, :] + rotation) % top, axis=1)


def portions_of(amount, total, limit, lean, full):
    portions = [(1 << 20) // math.isqrt(rank ** lean) + 1 for rank in range(1, amount + 1)]
    largest = limit if full else min(limit, max(-(-total // amount), total * portions[0] // sum(portions)))
    least = 1 if total - largest >= amount - 1 else 0
    holding, surplus = [largest] + [least] * (amount - 1), total - largest - least * (amount - 1)
    while surplus > 0:
        candidates = [i for i in range(1, amount) if holding[i] < largest] or [i for i in range(1, amount) if holding[i] < limit]
        pool, remaining = sum([portions[i] for i in candidates]), surplus
        for i in candidates:
            addition = min(limit - holding[i], max(1, remaining * portions[i] // pool), surplus)
            holding[i] = holding[i] + addition
            surplus = surplus - addition
    return np.array(holding)


def normal_values(rng, extent, scale, bound, shards=(), kind=jnp.bfloat16):
    array = scale * jax.random.normal(rng, extent, jnp.float32)
    if shards:
        array = array * levels(rng, extent, shards, -0.22, 0.18)
    return jnp.clip(array, -bound, bound).astype(kind)


def setup_inputs(seed: int = 0) -> dict:
    arg_keys = jax.random.split(jax.random.key(seed), 18)
    residual_in = normal_values(arg_keys[0], (TOKENS, D), 1.0, 6.0, ((0, 128),))
    gla_state = normal_values(arg_keys[1], (TOKENS, HEADS, DKH, DVH), 1.0, 6.0, ((0, 128), (1, 4)), jnp.float32)
    norm_gain = jnp.clip(1.0 + 0.18 * jax.random.normal(arg_keys[2], (D,), jnp.float32), 0.099609375, 1.8984375).astype(jnp.bfloat16)
    w_query = normal_values(arg_keys[3], (D, DK), D ** -0.5, 0.125, ((0, 128), (1, 4)))
    w_key = normal_values(arg_keys[4], (D, DK), D ** -0.5, 0.125, ((0, 128), (1, 4)))
    w_value = normal_values(arg_keys[5], (D, DV), D ** -0.5, 0.125, ((0, 128), (1, 4)))
    w_decay = normal_values(arg_keys[6], (D, DK), (4 * D ** -0.5), 0.5, ((0, 128), (1, 4)))
    decay_bias = draw_decay_bias(jax.random.fold_in(arg_keys[17], 71), 0)
    head_gain = jnp.clip(1.0 + 0.18 * jax.random.normal(arg_keys[8], (DVH,), jnp.float32), 0.099609375, 1.8984375).astype(jnp.bfloat16)
    w_output = normal_values(arg_keys[9], (DV, D), DV ** -0.5, 0.125, ((0, 4), (1, 128)))
    ffn_gain = jnp.clip(1.0 + 0.18 * jax.random.normal(arg_keys[10], (D,), jnp.float32), 0.099609375, 1.8984375).astype(jnp.bfloat16)
    router_group = normal_values(arg_keys[11], (D, GROUPS), D ** -0.5, 0.125)
    router_expert = normal_values(arg_keys[12], (EXPERTS, D), D ** -0.5, 0.125)
    expert_ids_keys = jax.random.split(jax.random.fold_in(arg_keys[13], 1), TOKENS // TOKENS)
    expert_ids_turns = jax.random.permutation(jax.random.fold_in(arg_keys[13], 3), TOKENS // TOKENS)
    expert_ids = jax.vmap(lambda own, number: deal_out(jax.random.fold_in(arg_keys[13], 2), own, number, TOKENS, EXPERTS, TOP, CAP, 2))(expert_ids_keys, expert_ids_turns).reshape((TOKENS, TOP))
    w_gate = normal_values(arg_keys[14], (EXPERTS, D, FF), D ** -0.5, 0.125, ((0, 128), (2, 4)))
    w_up = normal_values(arg_keys[15], (EXPERTS, D, FF), D ** -0.5, 0.125, ((0, 128), (2, 4)))
    w_down = normal_values(arg_keys[16], (EXPERTS, FF, D), (3 * FF ** -0.5), 0.75, ((0, 128), (1, 4)))
    return {"residual_in": residual_in, "gla_state": gla_state, "norm_gain": norm_gain, "w_query": w_query, "w_key": w_key, "w_value": w_value, "w_decay": w_decay, "decay_bias": decay_bias, "head_gain": head_gain, "w_output": w_output, "ffn_gain": ffn_gain, "router_group": router_group, "router_expert": router_expert, "expert_ids": expert_ids, "w_gate": w_gate, "w_up": w_up, "w_down": w_down}


EPSILON = 1e-06
GATE_SCALE = 16.0

def rms_scale(values, gain_vec):
    floats = values.astype(jnp.float32)
    return floats * lax.rsqrt(lax.optimization_barrier(jnp.mean(floats * floats, axis=-1, keepdims=True)) + EPSILON) * gain_vec.astype(jnp.float32)

def reference(residual_in, gla_state, norm_gain, w_query, w_key, w_value, w_decay, decay_bias, head_gain, w_output, ffn_gain, router_group, router_expert, expert_ids, w_gate, w_up, w_down):
    tokens = residual_in.shape[0]
    normed = rms_scale(residual_in, norm_gain).astype(jnp.bfloat16)
    query_rows = jnp.dot(normed, w_query, preferred_element_type=jnp.float32).astype(jnp.bfloat16)
    key_rows = jnp.dot(normed, w_key, preferred_element_type=jnp.float32).astype(jnp.bfloat16)
    value_rows = jnp.dot(normed, w_value, preferred_element_type=jnp.float32).astype(jnp.bfloat16)
    decay_pre = jnp.dot(normed, w_decay, preferred_element_type=jnp.float32)
    log_decay = jax.nn.log_sigmoid(decay_pre + decay_bias) / GATE_SCALE
    query_float = lax.optimization_barrier(query_rows).astype(jnp.float32).reshape(tokens, HEADS, DKH) * DKH ** (-0.5)
    key_float = lax.optimization_barrier(key_rows).astype(jnp.float32).reshape(tokens, HEADS, DKH)
    value_float = lax.optimization_barrier(value_rows).astype(jnp.float32).reshape(tokens, HEADS, DVH)
    alpha = jnp.exp(log_decay).reshape(tokens, HEADS, DKH)
    new_state = alpha[..., None] * gla_state + key_float[..., None] * value_float[:, :, None, :]
    read_out = jnp.einsum('thk,thkv->thv', query_float, new_state, precision=lax.Precision.HIGHEST)
    gated_heads = rms_scale(read_out, head_gain).astype(jnp.bfloat16)
    attention = jnp.zeros((tokens, D), jnp.float32)
    for head_index in range(HEADS):
        partial_out = jnp.dot(gated_heads[:, head_index], w_output[head_index * DVH:(head_index + 1) * DVH], preferred_element_type=jnp.float32).astype(jnp.bfloat16)
        attention = attention + lax.optimization_barrier(partial_out).astype(jnp.float32)
    hidden_res = (residual_in.astype(jnp.float32) + attention).astype(jnp.bfloat16)
    moe_in = rms_scale(hidden_res, ffn_gain).astype(jnp.bfloat16)
    group_logits = jnp.dot(moe_in, router_group, preferred_element_type=jnp.float32)
    expert_logits = jnp.dot(moe_in, router_expert.T, preferred_element_type=jnp.float32)
    per_group = EXPERTS // GROUPS

    def route_weight(mine_col, other_col):
        chosen = jnp.take_along_axis(expert_logits, expert_ids[:, mine_col:mine_col + 1], axis=1)[:, 0]
        rival_logit = jnp.take_along_axis(expert_logits, expert_ids[:, other_col:other_col + 1], axis=1)[:, 0]
        group_of = (expert_ids[:, mine_col] // per_group).astype(jnp.int32)
        group_logit = jnp.take_along_axis(group_logits, group_of[:, None], axis=1)[:, 0]
        group_share = 1.0 / lax.optimization_barrier(jnp.sum(jnp.exp(group_logits - group_logit[:, None]), axis=1))
        return group_share * jax.nn.sigmoid(chosen - rival_logit)
    weights = jnp.stack([route_weight(0, 1), route_weight(1, 0)], axis=1)
    slot_index = jnp.arange(CAP, dtype=jnp.int32)

    def expert_step(summed, expert):
        is_named = jnp.any(expert_ids == expert, axis=1)
        slot_of = jnp.cumsum(is_named.astype(jnp.int32)) - 1
        select = (is_named[None, :] & (slot_of[None, :] == slot_index[:, None])).astype(jnp.float32)
        slot_rows = jnp.dot(select.astype(jnp.bfloat16), moe_in, preferred_element_type=jnp.float32).astype(jnp.bfloat16)
        gate_out = jnp.dot(slot_rows, w_gate[expert], preferred_element_type=jnp.float32)
        up_out = jnp.dot(slot_rows, w_up[expert], preferred_element_type=jnp.float32)
        hidden = (jax.nn.silu(gate_out) * up_out).astype(jnp.bfloat16)
        output = jnp.dot(hidden, w_down[expert], preferred_element_type=jnp.float32)
        token_weight = lax.optimization_barrier(jnp.sum(jnp.where(expert_ids == expert, weights, jnp.zeros_like(weights)), axis=1))
        slot_weight = jnp.dot(select, token_weight, precision=lax.Precision.HIGHEST)
        summed = summed + jnp.dot(select.T, output * slot_weight[:, None], precision=lax.Precision.HIGHEST)
        return (summed, None)
    moe_sum, _ = lax.scan(expert_step, jnp.zeros((tokens, D), jnp.float32), jnp.arange(EXPERTS, dtype=jnp.int32))
    layer_out = (hidden_res.astype(jnp.float32) + moe_sum).astype(jnp.bfloat16)
    return (layer_out, new_state)
```

```python
import functools
import types

import jax
import jax.numpy as jnp
from jax import lax
from jax.experimental import pallas as pl
from jax.experimental.pallas import tpu as pltpu
from jax.sharding import Mesh
from jax.sharding import PartitionSpec as P

CAP = 16
EPSILON = 1e-06
GATE_SCALE = 16.0
AXES = ("z", "y", "c", "x")
EP = ("z", "y", "c")
MESH = pl.DeviceIdType.MESH
BF16 = jnp.bfloat16
F32 = jnp.float32

(
    PROJ_W,
    PROJ_T,
    OUT_W,
    PROJ_SUM,
    HEADS,
    HEAD_SUM,
    GATHER,
    PICKED,
    GATE_W,
    DOWN_W,
    GATE_SUM,
    MERGE,
    COMBINE,
    QUARTERS,
    EXCHANGES,
) = range(15)


def rounds(n, offset):
    return min(offset % n, -offset % n)


def rms_scale(values, gain):
    mean = jnp.mean(values * values, axis=-1, keepdims=True)
    return values * lax.rsqrt(mean + EPSILON) * gain


def matmul(a, b):
    return jnp.dot(a, b, preferred_element_type=F32)


def matmul_t(a, b):
    return lax.dot_general(a, b, (((1,), (1,)), ((), ())), preferred_element_type=F32)


def layer_kernel(
    s,
    residual,
    norm_gain,
    w_query,
    w_key,
    w_value,
    w_decay,
    decay_bias,
    state,
    head_gain,
    w_output_t,
    ffn_gain,
    router_group_t,
    router_expert,
    ids_t,
    w_gate,
    w_up,
    w_down,
    layer_out,
    alpha_out,
    key_out,
    value_out,
    v_residual,
    v_norm_gain,
    v_bias,
    v_head_gain,
    v_ffn_gain,
    v_ids,
    v_state,
    v_router,
    v_group,
    w_own,
    w_row,
    normed_out,
    normed_in,
    out_w,
    sums_out,
    sums_in,
    heads,
    head_out,
    head_in,
    moe_in,
    hidden_q,
    gathered,
    picked_out,
    picked_in,
    gate_w,
    down_w,
    partial,
    merge_out,
    merge_in,
    combine_out,
    combine_in,
    quarters,
    v_alpha,
    v_key,
    v_value,
    v_layer,
    load_sem,
    store_sem,
    send_sem,
    recv_sem,
    plane_sem,
):
    z, y, c, x = (lax.axis_index(a) for a in AXES)
    other_c = 1 - c
    row = y * s.C + c
    plane = z * s.Y + y
    expert = plane * s.C + c
    half_w = s.half

    def at(dz=0, dy=0, dc=0, dx=0):
        return (
            lax.rem(z + dz, s.Z) if dz else z,
            lax.rem(y + dy, s.Y) if dy else y,
            lax.rem(c + dc, s.C) if dc else c,
            lax.rem(x + dx, s.X) if dx else x,
        )

    def ordered(offsets):
        def far(o):
            return -(rounds(s.Z, o[0]) + rounds(s.Y, o[1]) + rounds(s.X, o[3]))

        return sorted((o for o in offsets if any(o)), key=far)

    z_c = ordered((i, 0, k, 0) for i in range(s.Z) for k in range(s.C))
    y_c = ordered((0, i, k, 0) for i in range(s.Y) for k in range(s.C))
    z_only = ordered((i, 0, 0, 0) for i in range(s.Z))
    z_x = ordered((i, 0, 0, j) for i in range(s.Z) for j in range(s.X))
    z_y = ordered((i, j, 0, 0) for i in range(s.Z) for j in range(s.Y))
    x_only = ordered((0, 0, 0, i) for i in range(s.X))
    partner = at(dc=1)

    def send(which, src, dst, device):
        pltpu.make_async_remote_copy(
            src_ref=src,
            dst_ref=dst,
            send_sem=send_sem.at[which],
            recv_sem=recv_sem.at[which],
            device_id=device,
            device_id_type=MESH,
        ).start()

    def all_of(which, ref):
        return pltpu.make_async_remote_copy(
            src_ref=ref,
            dst_ref=ref,
            send_sem=send_sem.at[which],
            recv_sem=recv_sem.at[which],
            device_id=partner,
            device_id_type=MESH,
        )

    loads = []

    def load(src, dst):
        copy = pltpu.make_async_copy(src, dst, load_sem.at[len(loads)])
        loads.append(copy)
        copy.start()
        return copy

    k = s.dkh
    ld_weights = [
        load(w_query, w_own.at[0, :, pl.ds(0, k)]),
        load(w_key, w_own.at[0, :, pl.ds(k, k)]),
        load(w_decay.at[:, pl.ds(0, k // 2)], w_own.at[0, :, pl.ds(2 * k, k // 2)]),
        load(w_decay.at[:, pl.ds(k // 2, k // 2)], w_own.at[1, :, pl.ds(0, k // 2)]),
        load(w_value, w_own.at[1, :, pl.ds(k // 2, s.dvh)]),
    ]
    ld_residual = [load(residual, v_residual), load(norm_gain, v_norm_gain)]
    ld_ids = load(ids_t, v_ids)
    own_rows = pl.ds(pl.multiple_of(row * s.rows, s.rows), s.rows)
    own_q = pl.ds(pl.multiple_of(x * s.dq, s.dq), s.dq)
    own_f = pl.ds(pl.multiple_of(x * s.fh, s.fh), s.fh)
    own_f2 = pl.ds(pl.multiple_of(s.ff + x * s.fh, s.fh), s.fh)
    ld_state = [load(decay_bias, v_bias), load(head_gain, v_head_gain), load(state, v_state)]
    ld_out_w = [load(w_output_t, out_w.at[own_rows, :])]
    ld_ffn = [load(ffn_gain, v_ffn_gain)]
    ld_moe = [
        load(w_gate.at[own_q, :], gate_w.at[:, own_f]),
        load(w_up.at[own_q, :], gate_w.at[:, own_f2]),
        load(w_down.at[:, own_q], down_w.at[own_f, :]),
        load(router_expert.at[:, own_q], v_router),
        load(router_group_t.at[:, own_q], v_group),
    ]

    barrier = pltpu.get_barrier_semaphore()
    greeted = y_c + z_c[:] + x_only
    greeted = list(dict.fromkeys(greeted))
    for o in greeted:
        pl.semaphore_signal(barrier, inc=1, device_id=at(*o), device_id_type=MESH)

    for copy in ld_residual:
        copy.wait()
    normed = rms_scale(v_residual[...].astype(F32), v_norm_gain[...].astype(F32)).astype(BF16)
    for i in range(s.Z):
        normed_out[i] = normed[:, i * s.zb : (i + 1) * s.zb]
    for copy in ld_weights:
        copy.wait()

    pl.semaphore_wait(barrier, len(greeted))

    for o in y_c:
        to = at(*o)
        send(PROJ_W, w_own.at[to[2]], w_row.at[own_rows, :], to)
    for o in z_c:
        to = at(*o)
        send(PROJ_T, normed_out.at[to[0]], normed_in.at[z * s.C + c], to)
    for o in z_only:
        pl.semaphore_signal(plane_sem, inc=1, device_id=at(*o), device_id_type=MESH)
    ld_out_w[0].wait()
    for o in y_c:
        to = at(*o)
        send(OUT_W, out_w.at[own_rows, :], out_w.at[own_rows, :], to)
    for o in x_only:
        to = at(*o)
        their_q = pl.ds(pl.multiple_of(to[3] * s.dq, s.dq), s.dq)
        send(GATE_W, w_gate.at[their_q, :], gate_w.at[:, own_f], to)
        send(GATE_W, w_up.at[their_q, :], gate_w.at[:, own_f2], to)
    for o in x_only:
        to = at(*o)
        their_q = pl.ds(pl.multiple_of(to[3] * s.dq, s.dq), s.dq)
        send(DOWN_W, w_down.at[:, their_q], down_w.at[own_f, :], to)

    normed_in[z * s.C + c] = normed_out[z]
    w_row[own_rows, :] = w_own[c]

    ld_ids.wait()
    tokens = s.tokens
    ids = v_ids[...]
    first, second = ids[0:1], ids[1:2]
    partner_expert = plane * s.C + other_c
    own_named = ((first == expert) | (second == expert)).astype(F32)
    par_named = ((first == partner_expert) | (second == partner_expert)).astype(F32)
    named = jnp.concatenate([own_named, par_named, jnp.zeros((6, tokens), F32)], axis=0)
    t_row = lax.broadcasted_iota(jnp.int32, (tokens, tokens), 0)
    t_col = lax.broadcasted_iota(jnp.int32, (tokens, tokens), 1)
    upto = (t_row <= t_col).astype(BF16)
    code = named * matmul(named.astype(BF16), upto)
    slot_full = lax.broadcasted_iota(jnp.int32, (CAP, tokens), 0).astype(F32) + 1.0
    rival = jnp.where(first == expert, second, first).astype(F32)
    own_full = jnp.where(slot_full == code[0:1], 1.0, 0.0)
    rival_id = jnp.sum(own_full * rival, axis=1, keepdims=True).astype(jnp.int32)
    side = tokens // 2
    p_row = lax.broadcasted_iota(jnp.int32, (tokens, side), 0)
    p_col = lax.broadcasted_iota(jnp.int32, (tokens, side), 1)
    p_tok = 2 * p_col - lax.rem(p_col, 2)
    slot_side = lax.broadcasted_iota(jnp.int32, (CAP, side), 0).astype(F32) + 1.0
    code_c = matmul(code.astype(BF16), (p_row == p_tok + 2 * c).astype(BF16))
    code_o = matmul(code.astype(BF16), (p_row == p_tok + 2 * other_c).astype(BF16))
    own_here = (slot_side == code_c[0:1]).astype(F32)
    par_here = (slot_side == code_c[1:2]).astype(F32)
    own_there = (slot_side == code_o[0:1]).astype(F32)
    own_here_t = own_here.T.astype(BF16)
    own_there_t = own_there.T.astype(BF16)

    all_of(PROJ_T, normed_in.at[pl.ds(0, len(z_c))]).wait_recv()
    all_of(PROJ_W, w_row.at[pl.ds(0, len(y_c) * s.rows), :]).wait_recv()
    lines = s.Z * s.C
    sums = matmul(normed_in[...].reshape(2 * lines, s.zb), w_row[...])
    sums_out[...] = sums.astype(BF16).reshape(lines, 2, half_w)
    for o in z_c:
        to = at(*o)
        send(PROJ_SUM, sums_out.at[to[0] * s.C + to[2]], sums_in.at[c, z], to)
    sums_in[c, z] = sums_out[z * s.C + c]

    for copy in ld_state:
        copy.wait()
    all_of(PROJ_SUM, sums_out.at[pl.ds(0, len(z_c))]).wait_recv()
    low = jnp.sum(sums_in[0].astype(F32), axis=0)
    high = jnp.sum(sums_in[1].astype(F32), axis=0)
    query = low[:, :k].astype(BF16).astype(F32) * k ** (-0.5)
    key = low[:, k : 2 * k].astype(BF16).astype(F32)
    decay = jnp.concatenate([low[:, 2 * k :], high[:, : k // 2]], axis=1) + v_bias[...]
    value = high[:, k // 2 :].astype(BF16).astype(F32)
    log_decay = jnp.minimum(decay, 0.0) - jnp.log1p(jnp.exp(-jnp.abs(decay)))
    alpha = jnp.exp(log_decay / GATE_SCALE)
    query_alpha = jnp.concatenate([query * alpha, jnp.zeros((6, k), F32)], axis=0).T
    read_out = jnp.concatenate(
        [
            jnp.sum(query_alpha[:, 0:1] * v_state[0], axis=0, keepdims=True),
            jnp.sum(query_alpha[:, 1:2] * v_state[1], axis=0, keepdims=True),
        ],
        axis=0,
    )
    read_out = read_out + jnp.sum(query * key, axis=1, keepdims=True) * value
    heads[z] = rms_scale(read_out, v_head_gain[...].astype(F32)).astype(BF16)
    for o in z_only:
        send(HEADS, heads.at[z], heads.at[z], at(*o))
    v_alpha[...] = alpha
    v_key[...] = key
    v_value[...] = value
    stores = [
        pltpu.make_async_copy(v_alpha, alpha_out, store_sem.at[0]),
        pltpu.make_async_copy(v_key, key_out, store_sem.at[1]),
        pltpu.make_async_copy(v_value, value_out, store_sem.at[2]),
    ]
    for copy in stores:
        copy.start()

    pl.semaphore_wait(plane_sem, len(z_only))
    all_of(OUT_W, out_w.at[pl.ds(0, len(y_c) * s.rows), :]).wait_recv()
    all_of(HEADS, heads.at[pl.ds(0, len(z_only))]).wait_recv()
    part = matmul_t(heads[...].reshape(2 * s.Z, s.dvh), out_w[...])
    head_out[...] = part.astype(BF16).reshape(s.Z, 2, s.zb)
    for o in z_x:
        to = at(*o)
        send(HEAD_SUM, head_out.at[to[0]], head_in.at[z * s.X + x], to)
    head_in[z * s.X + x] = head_out[z]
    for copy in ld_ffn:
        copy.wait()
    all_of(HEAD_SUM, head_in.at[pl.ds(0, len(z_x))]).wait_recv()
    blocks = []
    for i in range(s.Z):
        total = head_in[i * s.X].astype(F32)
        for j in range(1, s.X):
            total = total + head_in[i * s.X + j].astype(F32)
        blocks.append(total)
    hidden_res = v_residual[...].astype(F32) + jnp.concatenate(blocks, axis=1)
    hidden_res = hidden_res.astype(BF16).astype(F32)
    moe_rows = rms_scale(hidden_res, v_ffn_gain[...].astype(F32)).astype(BF16)
    for i in range(s.X):
        moe_in[i] = moe_rows[:, i * s.dq : (i + 1) * s.dq]
        hidden_q[i] = hidden_res[:, i * s.dq : (i + 1) * s.dq]

    gathered[plane] = moe_in[x]
    for o in z_y:
        send(GATHER, moe_in.at[x], gathered.at[plane], at(*o))
    for copy in ld_moe:
        copy.wait()
    all_of(GATHER, gathered.at[pl.ds(0, len(z_y))]).wait_recv()
    rows = gathered[...].reshape(side, s.dq)
    picked_out[...] = matmul(par_here.astype(BF16), rows).astype(BF16)
    send(PICKED, picked_out, picked_in, partner)
    picked = matmul(own_here.astype(BF16), rows)
    all_of(GATE_W, gate_w.at[:, pl.ds(0, 2 * len(x_only) * s.fh)]).wait_recv()
    all_of(PICKED, picked_in).wait_recv()
    picked = (picked + picked_in[...].astype(F32)).astype(BF16)
    wide = 2 * s.ff
    partial[x, :, 0:wide] = matmul(picked, gate_w[...]).astype(BF16)
    partial[x, :, wide : wide + s.experts] = matmul_t(picked, v_router[...]).astype(BF16)
    groups = matmul_t(picked, v_group[...]).astype(BF16)
    partial[x, :, wide + s.experts : wide + s.experts + s.groups] = groups
    for o in x_only:
        send(GATE_SUM, partial.at[x], partial.at[x], at(*o))
    all_of(DOWN_W, down_w.at[pl.ds(0, len(x_only) * s.fh), :]).wait_recv()
    all_of(GATE_SUM, partial.at[pl.ds(0, len(x_only))]).wait_recv()
    both = jnp.sum(partial[:, :, 0:wide].astype(F32), axis=0)
    gate, up = both[:, : s.ff], both[:, s.ff :]
    hidden = (gate * (1.0 / (1.0 + jnp.exp(-gate))) * up).astype(BF16)
    output = matmul(hidden, down_w[...])
    logits = jnp.sum(partial[:, :, wide : wide + s.experts].astype(F32), axis=0)
    groups = jnp.sum(
        partial[:, :, wide + s.experts : wide + s.experts + s.groups].astype(F32), axis=0
    )
    lane = lax.broadcasted_iota(jnp.int32, logits.shape, 1)
    chosen = jnp.sum(jnp.where(lane == expert, logits, 0.0), axis=1, keepdims=True)
    against = jnp.sum(jnp.where(lane == rival_id, logits, 0.0), axis=1, keepdims=True)
    g_lane = lax.broadcasted_iota(jnp.int32, groups.shape, 1)
    own_group = lax.div(expert, s.experts // s.groups)
    g_own = jnp.sum(jnp.where(g_lane == own_group, groups, 0.0), axis=1, keepdims=True)
    share = 1.0 / jnp.sum(jnp.exp(groups - g_own), axis=1, keepdims=True)
    weight = share * (1.0 / (1.0 + jnp.exp(against - chosen)))
    scaled = (output * weight).astype(BF16)

    merge_out[...] = matmul(own_there_t, scaled).astype(BF16)
    send(MERGE, merge_out, merge_in, partner)
    here = matmul(own_here_t, scaled)
    all_of(MERGE, merge_in).wait_recv()
    merged = (here + merge_in[...].astype(F32)).astype(BF16)
    combine_out[...] = merged.reshape(side // 2, 2, s.dq)
    for o in z_y:
        to = at(*o)
        send(COMBINE, combine_out.at[to[0] * s.Y + to[1]], combine_in.at[plane], to)
    combine_in[plane] = combine_out[plane]
    all_of(COMBINE, combine_in.at[pl.ds(0, len(z_y))]).wait_recv()
    moe_sum = jnp.sum(combine_in[...].astype(F32), axis=0)
    quarters[x] = (hidden_q[x] + moe_sum).astype(BF16)
    for o in x_only:
        send(QUARTERS, quarters.at[x], quarters.at[x], at(*o))
    all_of(QUARTERS, quarters.at[pl.ds(0, len(x_only))]).wait_recv()
    for i in range(s.X):
        v_layer[:, i * s.dq : (i + 1) * s.dq] = quarters[i]
    done = pltpu.make_async_copy(v_layer, layer_out, store_sem.at[3])
    done.start()

    all_of(PROJ_W, w_row.at[pl.ds(0, len(y_c) * s.rows), :]).wait_send()
    all_of(PROJ_T, normed_in.at[pl.ds(0, len(z_c))]).wait_send()
    all_of(OUT_W, out_w.at[pl.ds(0, len(y_c) * s.rows), :]).wait_send()
    all_of(PROJ_SUM, sums_out.at[pl.ds(0, len(z_c))]).wait_send()
    all_of(HEADS, heads.at[pl.ds(0, len(z_only))]).wait_send()
    all_of(HEAD_SUM, head_in.at[pl.ds(0, len(z_x))]).wait_send()
    all_of(GATHER, gathered.at[pl.ds(0, len(z_y))]).wait_send()
    all_of(PICKED, picked_out).wait_send()
    all_of(GATE_W, gate_w.at[:, pl.ds(0, 2 * len(x_only) * s.fh)]).wait_send()
    all_of(DOWN_W, down_w.at[pl.ds(0, len(x_only) * s.fh), :]).wait_send()
    all_of(GATE_SUM, partial.at[pl.ds(0, len(x_only))]).wait_send()
    all_of(MERGE, merge_out).wait_send()
    all_of(COMBINE, combine_in.at[pl.ds(0, len(z_y))]).wait_send()
    all_of(QUARTERS, quarters.at[pl.ds(0, len(x_only))]).wait_send()
    for copy in stores:
        copy.wait()
    done.wait()


def on_device(
    s,
    residual_in,
    gla_state,
    norm_gain,
    w_query,
    w_key,
    w_value,
    w_decay,
    decay_bias,
    head_gain,
    w_output,
    ffn_gain,
    router_group,
    router_expert,
    expert_ids,
    w_gate,
    w_up,
    w_down,
):
    old_state = gla_state[:, 0]
    side = s.tokens // 2
    vmem = pltpu.VMEM
    scratch = [
        vmem((2, s.d), BF16),
        vmem((1, s.d), BF16),
        vmem((1, s.dkh), F32),
        vmem((1, s.dvh), BF16),
        vmem((1, s.d), BF16),
        vmem((2, s.tokens), jnp.int32),
        vmem((2, s.dkh, s.dvh), F32),
        vmem((s.experts, s.dq), BF16),
        vmem((s.groups, s.dq), BF16),
        vmem((2, s.rows, s.half), BF16),
        vmem((s.zb, s.half), BF16),
        vmem((s.Z, 2, s.zb), BF16),
        vmem((s.Z * s.C, 2, s.zb), BF16),
        vmem((s.zb, s.dvh), BF16),
        vmem((s.Z * s.C, 2, s.half), BF16),
        vmem((2, s.Z, 2, s.half), BF16),
        vmem((s.Z, 2, s.dvh), BF16),
        vmem((s.Z, 2, s.zb), BF16),
        vmem((s.Z * s.X, 2, s.zb), BF16),
        vmem((s.X, 2, s.dq), BF16),
        vmem((s.X, 2, s.dq), F32),
        vmem((side // 2, 2, s.dq), BF16),
        vmem((CAP, s.dq), BF16),
        vmem((CAP, s.dq), BF16),
        vmem((s.dq, 2 * s.ff), BF16),
        vmem((s.ff, s.dq), BF16),
        vmem((s.X, CAP, 2 * s.ff + s.experts + 128), BF16),
        vmem((side, s.dq), BF16),
        vmem((side, s.dq), BF16),
        vmem((side // 2, 2, s.dq), BF16),
        vmem((side // 2, 2, s.dq), BF16),
        vmem((s.X, 2, s.dq), BF16),
        vmem((2, s.dkh), F32),
        vmem((2, s.dkh), F32),
        vmem((2, s.dvh), F32),
        vmem((2, s.d), BF16),
        pltpu.SemaphoreType.DMA((18,)),
        pltpu.SemaphoreType.DMA((4,)),
        pltpu.SemaphoreType.DMA((EXCHANGES,)),
        pltpu.SemaphoreType.DMA((EXCHANGES,)),
        pltpu.SemaphoreType.REGULAR,
    ]
    args = (
        residual_in,
        norm_gain[None],
        w_query,
        w_key,
        w_value,
        w_decay,
        decay_bias[None],
        old_state,
        head_gain[None],
        w_output.T,
        ffn_gain[None],
        router_group.T,
        router_expert,
        expert_ids.T,
        w_gate[0],
        w_up[0],
        w_down[0],
    )
    anywhere = pl.BlockSpec(memory_space=pl.ANY)
    layer_out, alpha, key, value = pl.pallas_call(
        functools.partial(layer_kernel, s),
        out_shape=(
            jax.ShapeDtypeStruct((2, s.d), BF16),
            jax.ShapeDtypeStruct((2, s.dkh), F32),
            jax.ShapeDtypeStruct((2, s.dkh), F32),
            jax.ShapeDtypeStruct((2, s.dvh), F32),
        ),
        in_specs=[anywhere] * len(args),
        out_specs=(anywhere,) * 4,
        scratch_shapes=scratch,
        compiler_params=pltpu.CompilerParams(collective_id=0, has_side_effects=True),
        name="layer",
    )(*args)
    new_state = alpha[:, :, None] * old_state + key[:, :, None] * value[:, None, :]
    return layer_out, new_state[:, None]


def build(torus, residual, state, w_gate, router_group):
    Z, Y, C, X = (torus.shape[a] for a in AXES)
    tokens, d = residual
    experts, _, ff = w_gate
    dkh, dvh = state[2], state[3]
    s = types.SimpleNamespace(
        Z=Z,
        Y=Y,
        C=C,
        X=X,
        tokens=tokens,
        d=d,
        rows=d // (Z * Y * C),
        zb=d // Z,
        dq=d // X,
        dkh=dkh,
        dvh=dvh,
        half=(3 * dkh + dvh) // 2,
        ff=ff,
        fh=ff // X,
        experts=experts,
        groups=router_group[1],
    )
    in_specs = (
        P(EP, None),
        P(EP, "x", None, None),
        P(),
        P(EP, "x"),
        P(EP, "x"),
        P(EP, "x"),
        P(EP, "x"),
        P("x"),
        P(),
        P("x", EP),
        P(),
        P(),
        P(),
        P(),
        P(EP, None, "x"),
        P(EP, None, "x"),
        P(EP, "x", None),
    )
    out_specs = (P(EP, None), P(EP, "x", None, None))
    return jax.shard_map(
        functools.partial(on_device, s),
        mesh=torus,
        in_specs=in_specs,
        out_specs=out_specs,
        check_vma=False,
    )


def solution(mesh):
    torus = Mesh(mesh.devices.reshape(8, 8, 2, mesh.shape["tp"]), AXES)

    def layer(*args):
        shapes = args[0].shape, args[1].shape, args[14].shape, args[11].shape
        return build(torus, *shapes)(*args)

    return layer
```

```python
import functools
import types

import jax
import jax.numpy as jnp
from jax import lax
from jax.experimental import pallas as pl
from jax.experimental.pallas import tpu as pltpu
from jax.sharding import Mesh
from jax.sharding import PartitionSpec as P

CAP = 16
EPSILON = 1e-06
GATE_SCALE = 16.0
AXES = ("z", "y", "c", "x")
EP = ("z", "y", "c")
MESH = pl.DeviceIdType.MESH
BF16 = jnp.bfloat16
F32 = jnp.float32

(
    PROJ_W,
    PROJ_T,
    OUT_W,
    PROJ_SUM,
    HEADS,
    HEAD_SUM,
    GATHER,
    PICKED,
    GATE_W,
    DOWN_W,
    GATE_SUM,
    MERGE,
    COMBINE,
    QUARTERS,
    EXCHANGES,
) = range(15)


def rounds(n, offset):
    return min(offset % n, -offset % n)


def rms_scale(values, gain):
    mean = jnp.mean(values * values, axis=-1, keepdims=True)
    return values * lax.rsqrt(mean + EPSILON) * gain


def matmul(a, b):
    return jnp.dot(a, b, preferred_element_type=F32)


def matmul_t(a, b):
    return lax.dot_general(a, b, (((1,), (1,)), ((), ())), preferred_element_type=F32)


def row_of(ref):
    return ref[...].astype(F32).reshape(1, ref.shape[0])


def store_kernel(layer, state, layer_out, state_out, sem):
    copies = [
        pltpu.make_async_copy(layer, layer_out, sem.at[0]),
        pltpu.make_async_copy(state, state_out, sem.at[1]),
    ]
    for copy in copies:
        copy.start()
    for copy in copies:
        copy.wait()


def layer_kernel(
    s,
    residual,
    norm_gain,
    w_query,
    w_key,
    w_value,
    w_decay,
    decay_bias,
    state,
    head_gain,
    w_output_t,
    ffn_gain,
    router_group_t,
    router_expert,
    ids_t,
    w_gate,
    w_up,
    w_down,
    layer_out,
    new_state,
    v_residual,
    v_norm_gain,
    v_bias,
    v_head_gain,
    v_ffn_gain,
    v_ids,
    v_state,
    v_router,
    v_group,
    w_own,
    w_row,
    normed_out,
    normed_in,
    out_w,
    sums_out,
    sums_in,
    heads,
    head_out,
    head_in,
    moe_in,
    hidden_q,
    gathered,
    picked_out,
    picked_in,
    gate_w,
    down_w,
    partial,
    merge_out,
    merge_in,
    combine_out,
    combine_in,
    quarters,
    load_sem,
    send_sem,
    recv_sem,
    plane_sem,
):
    z, y, c, x = (lax.axis_index(a) for a in AXES)
    other_c = 1 - c
    row = y * s.C + c
    plane = z * s.Y + y
    expert = plane * s.C + c
    half_w = s.half

    pair = lax.rem(y, 2)
    line = (z * 2 + pair) * s.C + c

    def at(dz=0, dy=0, dc=0, dx=0, across=0):
        return (
            lax.rem(z + dz, s.Z) if dz else z,
            y + 1 - 2 * pair if across else lax.rem(y + dy, s.Y) if dy else y,
            lax.rem(c + dc, s.C) if dc else c,
            lax.rem(x + dx, s.X) if dx else x,
        )

    def ordered(offsets):
        def far(o):
            return -(rounds(s.Z, o[0]) + rounds(s.Y, o[1]) + rounds(s.X, o[3]) + sum(o[4:]))

        return sorted((o for o in offsets if any(o)), key=far)

    z_p = ordered((i, 0, k, 0, p) for i in range(s.Z) for k in range(s.C) for p in range(2))
    y_w = ordered((0, i, k, 0) for i in range(0, s.Y, 2) for k in range(s.C))
    y_c = ordered((0, i, k, 0) for i in range(s.Y) for k in range(s.C))
    z_only = ordered((i, 0, 0, 0) for i in range(s.Z))
    z_x = ordered((i, 0, 0, j) for i in range(s.Z) for j in range(s.X))
    z_y = ordered((i, j, 0, 0) for i in range(s.Z) for j in range(s.Y))
    x_only = ordered((0, 0, 0, i) for i in range(s.X))
    partner = at(dc=1)

    def send(which, src, dst, device):
        pltpu.make_async_remote_copy(
            src_ref=src,
            dst_ref=dst,
            send_sem=send_sem.at[which],
            recv_sem=recv_sem.at[which],
            device_id=device,
            device_id_type=MESH,
        ).start()

    def all_of(which, ref):
        return pltpu.make_async_remote_copy(
            src_ref=ref,
            dst_ref=ref,
            send_sem=send_sem.at[which],
            recv_sem=recv_sem.at[which],
            device_id=partner,
            device_id_type=MESH,
        )

    loads = []

    def load(src, dst):
        copy = pltpu.make_async_copy(src, dst, load_sem.at[len(loads)])
        loads.append(copy)
        copy.start()
        return copy

    k = s.dkh
    ld_weights = [
        load(w_query, w_own.at[0, :, pl.ds(0, k)]),
        load(w_key, w_own.at[0, :, pl.ds(k, k)]),
        load(w_decay.at[:, pl.ds(0, k // 2)], w_own.at[0, :, pl.ds(2 * k, k // 2)]),
        load(w_decay.at[:, pl.ds(k // 2, k // 2)], w_own.at[1, :, pl.ds(0, k // 2)]),
        load(w_value, w_own.at[1, :, pl.ds(k // 2, s.dvh)]),
    ]
    ld_residual = [load(residual, v_residual), load(norm_gain, v_norm_gain)]
    ld_ids = load(ids_t, v_ids)
    own_rows = pl.ds(pl.multiple_of(row * s.rows, s.rows), s.rows)
    own_q = pl.ds(pl.multiple_of(x * s.dq, s.dq), s.dq)
    own_f = pl.ds(pl.multiple_of(x * s.fh, s.fh), s.fh)
    own_f2 = pl.ds(pl.multiple_of(s.ff + x * s.fh, s.fh), s.fh)
    ld_state = [load(decay_bias, v_bias), load(head_gain, v_head_gain), load(state, v_state)]
    w_row[...] = jnp.zeros_like(w_row)
    ld_out_w = [load(w_output_t, out_w.at[own_rows, :])]
    ld_ffn = [load(ffn_gain, v_ffn_gain)]
    ld_moe = [
        load(w_gate.at[own_q, :], gate_w.at[:, own_f]),
        load(w_up.at[own_q, :], gate_w.at[:, own_f2]),
        load(w_down.at[:, own_q], down_w.at[own_f, :]),
        load(router_expert.at[:, own_q], v_router),
        load(router_group_t.at[:, own_q], v_group),
    ]

    barrier = pltpu.get_barrier_semaphore()
    greeted = y_c + [o for o in z_p if o[0]] + x_only
    for o in greeted:
        pl.semaphore_signal(barrier, inc=1, device_id=at(*o), device_id_type=MESH)

    for copy in ld_weights:
        copy.wait()

    pl.semaphore_wait(barrier, len(greeted))

    for o in y_w:
        to = at(*o)
        send(PROJ_W, w_own.at[to[2]], w_row.at[own_rows, :], to)
    for copy in ld_residual:
        copy.wait()
    normed = rms_scale(v_residual[...].astype(F32), row_of(v_norm_gain)).astype(BF16)
    for i in range(s.Z):
        normed_out[i] = normed[:, i * s.zb : (i + 1) * s.zb]
    for o in z_p:
        to = at(*o)
        send(PROJ_T, normed_out.at[to[0]], normed_in.at[line], to)
    for o in z_only:
        pl.semaphore_signal(plane_sem, inc=1, device_id=at(*o), device_id_type=MESH)
    ld_out_w[0].wait()
    for o in y_c:
        to = at(*o)
        send(OUT_W, out_w.at[own_rows, :], out_w.at[own_rows, :], to)
    for o in x_only:
        to = at(*o)
        their_q = pl.ds(pl.multiple_of(to[3] * s.dq, s.dq), s.dq)
        send(GATE_W, w_gate.at[their_q, :], gate_w.at[:, own_f], to)
        send(GATE_W, w_up.at[their_q, :], gate_w.at[:, own_f2], to)
    for o in x_only:
        to = at(*o)
        their_q = pl.ds(pl.multiple_of(to[3] * s.dq, s.dq), s.dq)
        send(DOWN_W, w_down.at[:, their_q], down_w.at[own_f, :], to)

    normed_in[line] = normed_out[z]
    w_row[own_rows, :] = w_own[c]

    ld_ids.wait()
    tokens = s.tokens
    ids = v_ids[...]
    first, second = ids[0:1], ids[1:2]
    partner_expert = plane * s.C + other_c
    own_named = ((first == expert) | (second == expert)).astype(F32)
    par_named = ((first == partner_expert) | (second == partner_expert)).astype(F32)
    named = jnp.concatenate([own_named, par_named, jnp.zeros((6, tokens), F32)], axis=0)
    t_row = lax.broadcasted_iota(jnp.int32, (tokens, tokens), 0)
    t_col = lax.broadcasted_iota(jnp.int32, (tokens, tokens), 1)
    upto = (t_row <= t_col).astype(BF16)
    code = named * matmul(named.astype(BF16), upto)
    slot_full = lax.broadcasted_iota(jnp.int32, (CAP, tokens), 0).astype(F32) + 1.0
    rival = jnp.where(first == expert, second, first).astype(F32)
    own_full = jnp.where(slot_full == code[0:1], 1.0, 0.0)
    rival_id = jnp.sum(own_full * rival, axis=1, keepdims=True).astype(jnp.int32)
    side = tokens // 2
    p_row = lax.broadcasted_iota(jnp.int32, (tokens, side), 0)
    p_col = lax.broadcasted_iota(jnp.int32, (tokens, side), 1)
    p_tok = 2 * p_col - lax.rem(p_col, 2)
    slot_side = lax.broadcasted_iota(jnp.int32, (CAP, side), 0).astype(F32) + 1.0
    code_c = matmul(code.astype(BF16), (p_row == p_tok + 2 * c).astype(BF16))
    code_o = matmul(code.astype(BF16), (p_row == p_tok + 2 * other_c).astype(BF16))
    own_here = (slot_side == code_c[0:1]).astype(F32)
    par_here = (slot_side == code_c[1:2]).astype(F32)
    own_there = (slot_side == code_o[0:1]).astype(F32)
    own_here_t = own_here.T.astype(BF16)
    own_there_t = own_there.T.astype(BF16)

    all_of(PROJ_T, normed_in.at[pl.ds(0, len(z_p))]).wait_recv()
    all_of(PROJ_W, w_row.at[pl.ds(0, len(y_w) * s.rows), :]).wait_recv()
    lines = s.Z * 2 * s.C
    sums = matmul(normed_in[...].reshape(2 * lines, s.zb), w_row[...])
    sums_out[...] = sums.astype(BF16).reshape(lines, 2, half_w)
    for o in z_p:
        to = at(*o)
        to_line = (to[0] * 2 + lax.rem(to[1], 2)) * s.C + to[2]
        send(PROJ_SUM, sums_out.at[to_line], sums_in.at[c, z * 2 + pair], to)
    sums_in[c, z * 2 + pair] = sums_out[line]

    for copy in ld_state:
        copy.wait()
    all_of(PROJ_SUM, sums_out.at[pl.ds(0, len(z_p))]).wait_recv()
    low = jnp.sum(sums_in[0].astype(F32), axis=0)
    high = jnp.sum(sums_in[1].astype(F32), axis=0)
    query = low[:, :k].astype(BF16).astype(F32) * k ** (-0.5)
    key = low[:, k : 2 * k].astype(BF16).astype(F32)
    decay = jnp.concatenate([low[:, 2 * k :], high[:, : k // 2]], axis=1) + row_of(v_bias)
    value = high[:, k // 2 :].astype(BF16).astype(F32)
    log_decay = jnp.minimum(decay, 0.0) - jnp.log1p(jnp.exp(-jnp.abs(decay)))
    alpha = jnp.exp(log_decay / GATE_SCALE)
    factors = jnp.concatenate([query * alpha, alpha, key, jnp.zeros((2, k), F32)], axis=0).T
    read_out = jnp.concatenate(
        [
            jnp.sum(factors[:, 0:1] * v_state[0], axis=0, keepdims=True),
            jnp.sum(factors[:, 1:2] * v_state[1], axis=0, keepdims=True),
        ],
        axis=0,
    )
    read_out = read_out + jnp.sum(query * key, axis=1, keepdims=True) * value
    heads[z] = rms_scale(read_out, row_of(v_head_gain)).astype(BF16)
    for o in z_only:
        send(HEADS, heads.at[z], heads.at[z], at(*o))
    for i in range(2):
        carried = factors[:, 2 + i : 3 + i] * v_state[i]
        new_state[i] = carried + factors[:, 4 + i : 5 + i] * value[i : i + 1]

    pl.semaphore_wait(plane_sem, len(z_only))
    all_of(OUT_W, out_w.at[pl.ds(0, len(y_c) * s.rows), :]).wait_recv()
    all_of(HEADS, heads.at[pl.ds(0, len(z_only))]).wait_recv()
    part = matmul_t(heads[...].reshape(2 * s.Z, s.dvh), out_w[...])
    head_out[...] = part.astype(BF16).reshape(s.Z, 2, s.zb)
    for o in z_x:
        to = at(*o)
        send(HEAD_SUM, head_out.at[to[0]], head_in.at[z * s.X + x], to)
    head_in[z * s.X + x] = head_out[z]
    for copy in ld_ffn:
        copy.wait()
    all_of(HEAD_SUM, head_in.at[pl.ds(0, len(z_x))]).wait_recv()
    blocks = []
    for i in range(s.Z):
        total = head_in[i * s.X].astype(F32)
        for j in range(1, s.X):
            total = total + head_in[i * s.X + j].astype(F32)
        blocks.append(total)
    hidden_res = v_residual[...].astype(F32) + jnp.concatenate(blocks, axis=1)
    hidden_res = hidden_res.astype(BF16).astype(F32)
    moe_rows = rms_scale(hidden_res, row_of(v_ffn_gain)).astype(BF16)
    for i in range(s.X):
        moe_in[i] = moe_rows[:, i * s.dq : (i + 1) * s.dq]
        hidden_q[i] = hidden_res[:, i * s.dq : (i + 1) * s.dq]

    gathered[plane] = moe_in[x]
    for o in z_y:
        send(GATHER, moe_in.at[x], gathered.at[plane], at(*o))
    for copy in ld_moe:
        copy.wait()
    all_of(GATHER, gathered.at[pl.ds(0, len(z_y))]).wait_recv()
    rows = gathered[...].reshape(side, s.dq)
    picked_out[...] = matmul(par_here.astype(BF16), rows).astype(BF16)
    send(PICKED, picked_out, picked_in, partner)
    picked = matmul(own_here.astype(BF16), rows)
    all_of(GATE_W, gate_w.at[:, pl.ds(0, 2 * len(x_only) * s.fh)]).wait_recv()
    all_of(PICKED, picked_in).wait_recv()
    picked = (picked + picked_in[...].astype(F32)).astype(BF16)
    wide = 2 * s.ff
    partial[x, :, 0:wide] = matmul(picked, gate_w[...]).astype(BF16)
    partial[x, :, wide : wide + s.experts] = matmul_t(picked, v_router[...]).astype(BF16)
    groups = matmul_t(picked, v_group[...]).astype(BF16)
    partial[x, :, wide + s.experts : wide + s.experts + s.groups] = groups
    for o in x_only:
        send(GATE_SUM, partial.at[x], partial.at[x], at(*o))
    all_of(DOWN_W, down_w.at[pl.ds(0, len(x_only) * s.fh), :]).wait_recv()
    all_of(GATE_SUM, partial.at[pl.ds(0, len(x_only))]).wait_recv()
    both = jnp.sum(partial[:, :, 0:wide].astype(F32), axis=0)
    gate, up = both[:, : s.ff], both[:, s.ff :]
    hidden = (gate * (1.0 / (1.0 + jnp.exp(-gate))) * up).astype(BF16)
    output = matmul(hidden, down_w[...])
    logits = jnp.sum(partial[:, :, wide : wide + s.experts].astype(F32), axis=0)
    groups = jnp.sum(
        partial[:, :, wide + s.experts : wide + s.experts + s.groups].astype(F32), axis=0
    )
    lane = lax.broadcasted_iota(jnp.int32, logits.shape, 1)
    chosen = jnp.sum(jnp.where(lane == expert, logits, 0.0), axis=1, keepdims=True)
    against = jnp.sum(jnp.where(lane == rival_id, logits, 0.0), axis=1, keepdims=True)
    g_lane = lax.broadcasted_iota(jnp.int32, groups.shape, 1)
    own_group = lax.div(expert, s.experts // s.groups)
    g_own = jnp.sum(jnp.where(g_lane == own_group, groups, 0.0), axis=1, keepdims=True)
    share = 1.0 / jnp.sum(jnp.exp(groups - g_own), axis=1, keepdims=True)
    weight = share * (1.0 / (1.0 + jnp.exp(against - chosen)))
    scaled = (output * weight).astype(BF16)

    merge_out[...] = matmul(own_there_t, scaled).astype(BF16)
    send(MERGE, merge_out, merge_in, partner)
    here = matmul(own_here_t, scaled)
    all_of(MERGE, merge_in).wait_recv()
    merged = (here + merge_in[...].astype(F32)).astype(BF16)
    combine_out[...] = merged.reshape(side // 2, 2, s.dq)
    for o in z_y:
        to = at(*o)
        send(COMBINE, combine_out.at[to[0] * s.Y + to[1]], combine_in.at[plane], to)
    combine_in[plane] = combine_out[plane]
    all_of(COMBINE, combine_in.at[pl.ds(0, len(z_y))]).wait_recv()
    moe_sum = jnp.sum(combine_in[...].astype(F32), axis=0)
    quarters[x] = (hidden_q[x] + moe_sum).astype(BF16)
    for o in x_only:
        send(QUARTERS, quarters.at[x], quarters.at[x], at(*o))
    all_of(QUARTERS, quarters.at[pl.ds(0, len(x_only))]).wait_recv()
    for i in range(s.X):
        layer_out[:, i * s.dq : (i + 1) * s.dq] = quarters[i]

    all_of(PROJ_W, w_row.at[pl.ds(0, len(y_w) * s.rows), :]).wait_send()
    all_of(PROJ_T, normed_in.at[pl.ds(0, len(z_p))]).wait_send()
    all_of(OUT_W, out_w.at[pl.ds(0, len(y_c) * s.rows), :]).wait_send()
    all_of(PROJ_SUM, sums_out.at[pl.ds(0, len(z_p))]).wait_send()
    all_of(HEADS, heads.at[pl.ds(0, len(z_only))]).wait_send()
    all_of(HEAD_SUM, head_in.at[pl.ds(0, len(z_x))]).wait_send()
    all_of(GATHER, gathered.at[pl.ds(0, len(z_y))]).wait_send()
    all_of(PICKED, picked_out).wait_send()
    all_of(GATE_W, gate_w.at[:, pl.ds(0, 2 * len(x_only) * s.fh)]).wait_send()
    all_of(DOWN_W, down_w.at[pl.ds(0, len(x_only) * s.fh), :]).wait_send()
    all_of(GATE_SUM, partial.at[pl.ds(0, len(x_only))]).wait_send()
    all_of(MERGE, merge_out).wait_send()
    all_of(COMBINE, combine_in.at[pl.ds(0, len(z_y))]).wait_send()
    all_of(QUARTERS, quarters.at[pl.ds(0, len(x_only))]).wait_send()


def on_device(
    s,
    residual_in,
    gla_state,
    norm_gain,
    w_query,
    w_key,
    w_value,
    w_decay,
    decay_bias,
    head_gain,
    w_output,
    ffn_gain,
    router_group,
    router_expert,
    expert_ids,
    w_gate,
    w_up,
    w_down,
):
    old_state = gla_state[:, 0]
    side = s.tokens // 2
    vmem = pltpu.VMEM
    scratch = [
        vmem((2, s.d), BF16),
        vmem((s.d,), BF16),
        vmem((s.dkh,), F32),
        vmem((s.dvh,), BF16),
        vmem((s.d,), BF16),
        vmem((2, s.tokens), jnp.int32),
        vmem((2, s.dkh, s.dvh), F32),
        vmem((s.experts, s.dq), BF16),
        vmem((s.groups, s.dq), BF16),
        vmem((2, s.rows, s.half), BF16),
        vmem((s.zb, s.half), BF16),
        vmem((s.Z, 2, s.zb), BF16),
        vmem((s.Z * 2 * s.C, 2, s.zb), BF16),
        vmem((s.zb, s.dvh), BF16),
        vmem((s.Z * 2 * s.C, 2, s.half), BF16),
        vmem((2, s.Z * 2, 2, s.half), BF16),
        vmem((s.Z, 2, s.dvh), BF16),
        vmem((s.Z, 2, s.zb), BF16),
        vmem((s.Z * s.X, 2, s.zb), BF16),
        vmem((s.X, 2, s.dq), BF16),
        vmem((s.X, 2, s.dq), F32),
        vmem((side // 2, 2, s.dq), BF16),
        vmem((CAP, s.dq), BF16),
        vmem((CAP, s.dq), BF16),
        vmem((s.dq, 2 * s.ff), BF16),
        vmem((s.ff, s.dq), BF16),
        vmem((s.X, CAP, 2 * s.ff + s.experts + 128), BF16),
        vmem((side, s.dq), BF16),
        vmem((side, s.dq), BF16),
        vmem((side // 2, 2, s.dq), BF16),
        vmem((side // 2, 2, s.dq), BF16),
        vmem((s.X, 2, s.dq), BF16),
        pltpu.SemaphoreType.DMA((18,)),
        pltpu.SemaphoreType.DMA((EXCHANGES,)),
        pltpu.SemaphoreType.DMA((EXCHANGES,)),
        pltpu.SemaphoreType.REGULAR,
    ]
    args = (
        residual_in,
        norm_gain,
        w_query,
        w_key,
        w_value,
        w_decay,
        decay_bias,
        old_state,
        head_gain,
        w_output.T,
        ffn_gain,
        router_group.T,
        router_expert,
        expert_ids.T,
        w_gate[0],
        w_up[0],
        w_down[0],
    )
    anywhere = pl.BlockSpec(memory_space=pl.ANY)
    layer_out, new_state = pl.pallas_call(
        functools.partial(layer_kernel, s),
        out_shape=(pltpu.VMEM((2, s.d), BF16), pltpu.VMEM((2, s.dkh, s.dvh), F32)),
        in_specs=[anywhere] * len(args),
        out_specs=(pl.BlockSpec(memory_space=vmem),) * 2,
        scratch_shapes=scratch,
        compiler_params=pltpu.CompilerParams(collective_id=0, has_side_effects=True),
        name="layer",
    )(*args)
    held = [pltpu.with_memory_space_constraint(a, vmem) for a in (layer_out, new_state)]
    layer_out, new_state = pl.pallas_call(
        store_kernel,
        out_shape=(
            jax.ShapeDtypeStruct((2, s.d), BF16),
            jax.ShapeDtypeStruct((2, s.dkh, s.dvh), F32),
        ),
        in_specs=[pl.BlockSpec(memory_space=vmem)] * 2,
        out_specs=(anywhere,) * 2,
        scratch_shapes=[pltpu.SemaphoreType.DMA((2,))],
        compiler_params=pltpu.CompilerParams(vmem_limit_bytes=1 << 20),
        name="store",
    )(*held)
    return layer_out, new_state[:, None]


def build(torus, residual, state, w_gate, router_group):
    Z, Y, C, X = (torus.shape[a] for a in AXES)
    tokens, d = residual
    experts, _, ff = w_gate
    dkh, dvh = state[2], state[3]
    s = types.SimpleNamespace(
        Z=Z,
        Y=Y,
        C=C,
        X=X,
        tokens=tokens,
        d=d,
        rows=d // (Z * Y * C),
        zb=d // Z,
        dq=d // X,
        dkh=dkh,
        dvh=dvh,
        half=(3 * dkh + dvh) // 2,
        ff=ff,
        fh=ff // X,
        experts=experts,
        groups=router_group[1],
    )
    in_specs = (
        P(EP, None),
        P(EP, "x", None, None),
        P(),
        P(EP, "x"),
        P(EP, "x"),
        P(EP, "x"),
        P(EP, "x"),
        P("x"),
        P(),
        P("x", EP),
        P(),
        P(),
        P(),
        P(),
        P(EP, None, "x"),
        P(EP, None, "x"),
        P(EP, "x", None),
    )
    out_specs = (P(EP, None), P(EP, "x", None, None))
    return jax.shard_map(
        functools.partial(on_device, s),
        mesh=torus,
        in_specs=in_specs,
        out_specs=out_specs,
        check_vma=False,
    )


def solution(mesh):
    torus = Mesh(mesh.devices.reshape(8, 8, 2, mesh.shape["tp"]), AXES)

    def layer(*args):
        shapes = args[0].shape, args[1].shape, args[14].shape, args[11].shape
        return build(torus, *shapes)(*args)

    return layer
```

```python
import functools
import types

import jax
import jax.numpy as jnp
from jax import lax
from jax.experimental import pallas as pl
from jax.experimental.pallas import tpu as pltpu
from jax.sharding import Mesh
from jax.sharding import PartitionSpec as P

CAP = 16
EPSILON = 1e-06
GATE_SCALE = 16.0
AXES = ("z", "y", "c", "x")
EP = ("z", "y", "c")
MESH = pl.DeviceIdType.MESH
BF16 = jnp.bfloat16
F32 = jnp.float32

(
    PROJ_W,
    PROJ_T,
    RESIDUAL,
    OUT_W,
    OUT_PAIR,
    PROJ_SUM,
    HEADS,
    HEAD_SUM,
    GATHER,
    PICKED,
    GATE_W,
    DOWN_W,
    GATE_SUM,
    MERGE,
    COMBINE,
    QUARTERS,
    EXCHANGES,
) = range(17)


def rounds(n, offset):
    return min(offset % n, -offset % n)


def rms_scale(values, gain):
    mean = jnp.mean(values * values, axis=-1, keepdims=True)
    return values * lax.rsqrt(mean + EPSILON) * gain


def matmul(a, b):
    return jnp.dot(a, b, preferred_element_type=F32)


def matmul_t(a, b):
    return lax.dot_general(a, b, (((1,), (1,)), ((), ())), preferred_element_type=F32)


def row_of(ref):
    return ref[...].astype(F32).reshape(1, ref.shape[0])


def store_kernel(layer, state, layer_out, state_out, sem):
    copies = [
        pltpu.make_async_copy(layer, layer_out, sem.at[0]),
        pltpu.make_async_copy(state, state_out, sem.at[1]),
    ]
    for copy in copies:
        copy.start()
    for copy in copies:
        copy.wait()


def layer_kernel(
    s,
    residual,
    norm_gain,
    w_query,
    w_key,
    w_value,
    w_decay,
    decay_bias,
    state,
    head_gain,
    w_output_t,
    ffn_gain,
    router_group_t,
    router_expert,
    ids_t,
    w_gate,
    w_up,
    w_down,
    layer_out,
    new_state,
    v_residual,
    v_norm_gain,
    v_bias,
    v_head_gain,
    v_ffn_gain,
    v_ids,
    v_state,
    v_router,
    v_group,
    w_own,
    w_row,
    normed_out,
    normed_in,
    out_w,
    sums_out,
    sums_in,
    heads,
    head_out,
    head_in,
    residual_in,
    gathered,
    picked_out,
    picked_in,
    gate_w,
    down_w,
    partial,
    merge_out,
    merge_in,
    combine_out,
    combine_in,
    quarters,
    load_sem,
    send_sem,
    recv_sem,
    plane_sem,
):
    z, y, c, x = (lax.axis_index(a) for a in AXES)
    other_c = 1 - c
    row = y * s.C + c
    plane = z * s.Y + y
    expert = plane * s.C + c
    half_w = s.half

    pair = lax.rem(y, 2)
    line = (z * 2 + pair) * s.C + c

    z_pair = lax.rem(z, 2)
    block = lax.div(z, 2)

    def at(dz=0, dy=0, dc=0, dx=0, across=0, across_z=0):
        return (
            z + 1 - 2 * z_pair if across_z else lax.rem(z + dz, s.Z) if dz else z,
            y + 1 - 2 * pair if across else lax.rem(y + dy, s.Y) if dy else y,
            lax.rem(c + dc, s.C) if dc else c,
            lax.rem(x + dx, s.X) if dx else x,
        )

    def ordered(offsets):
        def far(o):
            return -(rounds(s.Z, o[0]) + rounds(s.Y, o[1]) + rounds(s.X, o[3]) + sum(o[4:]))

        return sorted((o for o in offsets if any(o)), key=far)

    z_p = ordered((i, 0, k, 0, p) for i in range(s.Z) for k in range(s.C) for p in range(2))
    y_w = ordered((0, i, k, 0) for i in range(0, s.Y, 2) for k in range(s.C))
    y_c = ordered((0, i, k, 0) for i in range(s.Y) for k in range(s.C))
    z_only = ordered((i, 0, 0, 0) for i in range(s.Z))
    z_even = ordered((i, 0, 0, 0) for i in range(0, s.Z, 2))
    out_from = ordered((0, i, 0, 0, 0, k) for i in range(s.Y) for k in range(2))
    z_y = ordered((i, j, 0, 0) for i in range(s.Z) for j in range(s.Y))
    x_only = ordered((0, 0, 0, i) for i in range(s.X))
    partner = at(dc=1)

    def send(which, src, dst, device):
        pltpu.make_async_remote_copy(
            src_ref=src,
            dst_ref=dst,
            send_sem=send_sem.at[which],
            recv_sem=recv_sem.at[which],
            device_id=device,
            device_id_type=MESH,
        ).start()

    def all_of(which, ref):
        return pltpu.make_async_remote_copy(
            src_ref=ref,
            dst_ref=ref,
            send_sem=send_sem.at[which],
            recv_sem=recv_sem.at[which],
            device_id=partner,
            device_id_type=MESH,
        )

    def side_of(its_z, its_y):
        return (lax.rem(its_z, 2) * s.Y + its_y) * s.blocks + lax.div(its_z, 2)

    loads = []

    def load(src, dst):
        copy = pltpu.make_async_copy(src, dst, load_sem.at[len(loads)])
        loads.append(copy)
        copy.start()
        return copy

    k = s.dkh
    ld_weights = [
        load(w_query, w_own.at[0, :, pl.ds(0, k)]),
        load(w_key, w_own.at[0, :, pl.ds(k, k)]),
        load(w_decay.at[:, pl.ds(0, k // 2)], w_own.at[0, :, pl.ds(2 * k, k // 2)]),
        load(w_decay.at[:, pl.ds(k // 2, k // 2)], w_own.at[1, :, pl.ds(0, k // 2)]),
        load(w_value, w_own.at[1, :, pl.ds(k // 2, s.dvh)]),
    ]
    ld_residual = [load(residual, v_residual), load(norm_gain, v_norm_gain)]
    ld_ids = load(ids_t, v_ids)
    own_rows = pl.ds(pl.multiple_of(row * s.rows, s.rows), s.rows)
    chunk = s.chunk
    wide_block = s.X * chunk

    def chunk_of(i, j):
        return pl.ds(pl.multiple_of(i * wide_block + j * chunk, chunk), chunk)

    own_f = pl.ds(pl.multiple_of(x * s.fh, s.fh), s.fh)
    own_f2 = pl.ds(pl.multiple_of(s.ff + x * s.fh, s.fh), s.fh)
    ld_state = [load(decay_bias, v_bias), load(head_gain, v_head_gain), load(state, v_state)]
    w_row[...] = jnp.zeros_like(w_row)
    v_group[...] = jnp.zeros_like(v_group)
    out_slot = z_pair * s.Y + y
    ld_out_w = [load(w_output_t, out_w.at[out_slot, c])]
    ld_ffn = [load(ffn_gain, v_ffn_gain)]
    ld_moe = [
        load(w_gate.at[:, x], gate_w.at[:, :, own_f]),
        load(w_up.at[:, x], gate_w.at[:, :, own_f2]),
    ]
    for i in range(s.blocks):
        cols = pl.ds(i * chunk, chunk)
        ld_moe.append(load(w_down.at[:, chunk_of(i, x)], down_w.at[own_f, cols]))
        ld_moe.append(load(router_expert.at[:, chunk_of(i, x)], v_router.at[:, cols]))
        ld_moe.append(
            load(router_group_t.at[:, chunk_of(i, x)], v_group.at[pl.ds(0, s.groups), cols])
        )

    barrier = pltpu.get_barrier_semaphore()
    greeted = y_c + [o for o in z_p if o[0]] + x_only + [o for o in out_from if o[1] and o[5]]
    for o in greeted:
        pl.semaphore_signal(barrier, inc=1, device_id=at(*o), device_id_type=MESH)

    for copy in ld_weights:
        copy.wait()

    pl.semaphore_wait(barrier, len(greeted))

    for o in y_w:
        to = at(*o)
        send(PROJ_W, w_own.at[to[2]], w_row.at[own_rows, :], to)
    for copy in ld_residual:
        copy.wait()
    normed = rms_scale(v_residual[...].astype(F32), row_of(v_norm_gain)).astype(BF16)
    for i in range(s.Z):
        normed_out[i] = normed[:, i * s.zb : (i + 1) * s.zb]
    for o in z_p:
        to = at(*o)
        send(PROJ_T, normed_out.at[to[0]], normed_in.at[line], to)
    for o in z_only:
        pl.semaphore_signal(plane_sem, inc=1, device_id=at(*o), device_id_type=MESH)
    for o in z_even:
        to = at(*o)
        theirs = chunk_of(lax.div(to[0], 2), x)
        send(RESIDUAL, v_residual.at[:, theirs], residual_in.at[block], to)
    ld_out_w[0].wait()
    for o in out_from:
        send(OUT_W, out_w.at[out_slot, c], out_w.at[out_slot, c], at(*o))
    for o in x_only:
        to = at(*o)
        send(GATE_W, w_gate.at[:, to[3]], gate_w.at[:, :, own_f], to)
        send(GATE_W, w_up.at[:, to[3]], gate_w.at[:, :, own_f2], to)
    for o in x_only:
        to = at(*o)
        for i in range(s.blocks):
            cols = pl.ds(i * chunk, chunk)
            send(DOWN_W, w_down.at[:, chunk_of(i, to[3])], down_w.at[own_f, cols], to)

    normed_in[line] = normed_out[z]
    residual_in[block] = v_residual[:, chunk_of(block, x)]
    w_row[own_rows, :] = w_own[c]

    for copy in ld_ffn:
        copy.wait()
    ld_ids.wait()
    tokens = s.tokens
    ids = v_ids[...]
    first, second = ids[0:1], ids[1:2]
    partner_expert = plane * s.C + other_c
    own_named = ((first == expert) | (second == expert)).astype(F32)
    par_named = ((first == partner_expert) | (second == partner_expert)).astype(F32)
    named = jnp.concatenate([own_named, par_named, jnp.zeros((6, tokens), F32)], axis=0)
    t_row = lax.broadcasted_iota(jnp.int32, (tokens, tokens), 0)
    t_col = lax.broadcasted_iota(jnp.int32, (tokens, tokens), 1)
    upto = (t_row <= t_col).astype(BF16)
    code = named * matmul(named.astype(BF16), upto)
    slot_full = lax.broadcasted_iota(jnp.int32, (CAP, tokens), 0).astype(F32) + 1.0
    rival = jnp.where(first == expert, second, first).astype(F32)
    own_full = jnp.where(slot_full == code[0:1], 1.0, 0.0)
    rival_id = jnp.sum(own_full * rival, axis=1, keepdims=True).astype(jnp.int32)
    side = tokens // 2
    p_row = lax.broadcasted_iota(jnp.int32, (tokens, side), 0)
    p_col = lax.broadcasted_iota(jnp.int32, (tokens, side), 1)
    per_z = s.Y * s.Z
    p_y = lax.div(lax.rem(p_col, per_z), s.Z)
    p_z = 2 * lax.div(lax.rem(p_col, s.Z), 2) + lax.div(p_col, per_z)
    p_tok = (p_z * s.Y + p_y) * 2 * s.C + lax.rem(p_col, 2)
    slot_side = lax.broadcasted_iota(jnp.int32, (CAP, side), 0).astype(F32) + 1.0
    code_c = matmul(code.astype(BF16), (p_row == p_tok + 2 * c).astype(BF16))
    code_o = matmul(code.astype(BF16), (p_row == p_tok + 2 * other_c).astype(BF16))
    own_here = (slot_side == code_c[0:1]).astype(F32)
    par_here = (slot_side == code_c[1:2]).astype(F32)
    own_there = (slot_side == code_o[0:1]).astype(F32)
    o_row = lax.broadcasted_iota(jnp.int32, (8, side), 0)
    o_col = lax.broadcasted_iota(jnp.int32, (8, side), 1)
    own_pick = (o_col == 2 * side_of(z, y) + o_row) & (o_row < 2)
    gains = row_of(v_ffn_gain)
    gain = jnp.zeros((1, s.dq), F32)
    for j in range(s.X):
        starts = [i * wide_block + j * chunk for i in range(s.blocks)]
        piece = jnp.concatenate([gains[:, a : a + chunk] for a in starts], axis=1)
        gain = gain + jnp.where(x == j, piece, 0.0)
    own_here_t = own_here.T.astype(BF16)
    own_there_t = own_there.T.astype(BF16)

    all_of(PROJ_T, normed_in.at[pl.ds(0, len(z_p))]).wait_recv()
    all_of(PROJ_W, w_row.at[pl.ds(0, len(y_w) * s.rows), :]).wait_recv()
    lines = s.Z * 2 * s.C
    sums = matmul(normed_in[...].reshape(2 * lines, s.zb), w_row[...])
    sums_out[...] = sums.astype(BF16).reshape(lines, 2, half_w)
    for o in z_p:
        to = at(*o)
        to_line = (to[0] * 2 + lax.rem(to[1], 2)) * s.C + to[2]
        send(PROJ_SUM, sums_out.at[to_line], sums_in.at[c, z * 2 + pair], to)
    sums_in[c, z * 2 + pair] = sums_out[line]

    for copy in ld_state:
        copy.wait()
    all_of(PROJ_SUM, sums_out.at[pl.ds(0, len(z_p))]).wait_recv()
    low = jnp.sum(sums_in[0].astype(F32), axis=0)
    high = jnp.sum(sums_in[1].astype(F32), axis=0)
    query = low[:, :k].astype(BF16).astype(F32) * k ** (-0.5)
    key = low[:, k : 2 * k].astype(BF16).astype(F32)
    decay = jnp.concatenate([low[:, 2 * k :], high[:, : k // 2]], axis=1) + row_of(v_bias)
    value = high[:, k // 2 :].astype(BF16).astype(F32)
    log_decay = jnp.minimum(decay, 0.0) - jnp.log1p(jnp.exp(-jnp.abs(decay)))
    alpha = jnp.exp(log_decay / GATE_SCALE)
    factors = jnp.concatenate([query * alpha, alpha, key, jnp.zeros((2, k), F32)], axis=0).T
    read_out = jnp.concatenate(
        [
            jnp.sum(factors[:, 0:1] * v_state[0], axis=0, keepdims=True),
            jnp.sum(factors[:, 1:2] * v_state[1], axis=0, keepdims=True),
        ],
        axis=0,
    )
    read_out = read_out + jnp.sum(query * key, axis=1, keepdims=True) * value
    heads[block] = rms_scale(read_out, row_of(v_head_gain)).astype(BF16)
    for o in z_even:
        send(HEADS, heads.at[block], heads.at[block], at(*o))
    all_of(OUT_W, out_w.at[pl.ds(0, len(out_from)), 0]).wait_recv()
    send(OUT_PAIR, out_w.at[:, c], out_w.at[:, c], partner)
    for i in range(2):
        carried = factors[:, 2 + i : 3 + i] * v_state[i]
        new_state[i] = carried + factors[:, 4 + i : 5 + i] * value[i : i + 1]

    all_of(RESIDUAL, residual_in.at[pl.ds(0, len(z_even))]).wait_recv()
    all_of(OUT_PAIR, out_w.at[:, 0]).wait_recv()
    all_of(HEADS, heads.at[pl.ds(0, len(z_even))]).wait_recv()
    part = matmul_t(heads[...].reshape(s.Z, s.dvh), out_w[...].reshape(wide_block, s.dvh))
    part = part.astype(BF16)
    for j in range(s.X):
        head_out[j] = part[:, j * chunk : (j + 1) * chunk]
    for o in x_only:
        to = at(*o)
        send(HEAD_SUM, head_out.at[to[3]], head_in.at[x], to)
    head_in[x] = head_out[x]
    pl.semaphore_wait(plane_sem, len(z_only))
    all_of(HEAD_SUM, head_in.at[pl.ds(0, len(x_only))]).wait_recv()
    attention = head_in[0].astype(F32)
    for j in range(1, s.X):
        attention = attention + head_in[j].astype(F32)
    residual_rows = residual_in[...].reshape(s.Z, chunk).astype(F32)
    gathered[plane] = (residual_rows + attention).astype(BF16)

    for o in z_y:
        send(GATHER, gathered.at[plane], gathered.at[plane], at(*o))
    for copy in ld_moe:
        copy.wait()
    all_of(GATHER, gathered.at[pl.ds(0, len(z_y))]).wait_recv()
    rows = jnp.concatenate(
        [
            gathered[pl.ds(2 * s.Y * i, 2 * s.Y)].reshape(side, chunk)
            for i in range(s.blocks)
        ],
        axis=1,
    )
    picked_out[...] = matmul(par_here.astype(BF16), rows).astype(BF16)
    send(PICKED, picked_out, picked_in, partner)
    picked = matmul(own_here.astype(BF16), rows)
    own_hidden = matmul(own_pick.astype(BF16), rows)
    all_of(GATE_W, gate_w.at[:, :, pl.ds(0, 2 * len(x_only) * s.fh)]).wait_recv()
    all_of(PICKED, picked_in).wait_recv()
    picked = picked + picked_in[...].astype(F32)
    square = jnp.sum(picked * picked, axis=1, keepdims=True)
    picked = (picked * gain).astype(BF16)
    wide = 2 * s.ff
    tail = wide + s.experts
    partial[x, :, 0:wide] = matmul(picked, gate_w[...].reshape(s.dq, wide)).astype(BF16)
    partial[x, :, wide:tail] = matmul_t(picked, v_router[...]).astype(BF16)
    groups = matmul_t(picked, v_group[...])
    g_lane = lax.broadcasted_iota(jnp.int32, groups.shape, 1)
    high = square.astype(BF16).astype(F32)
    groups = jnp.where(g_lane == s.groups, high, groups)
    groups = jnp.where(g_lane == s.groups + 1, square - high, groups)
    partial[x, :, tail : tail + 128] = groups.astype(BF16)
    for o in x_only:
        send(GATE_SUM, partial.at[x], partial.at[x], at(*o))
    all_of(DOWN_W, down_w.at[pl.ds(0, len(x_only) * s.fh), :]).wait_recv()
    all_of(GATE_SUM, partial.at[pl.ds(0, len(x_only))]).wait_recv()
    groups = jnp.sum(partial[:, :, tail : tail + 128].astype(F32), axis=0)
    squares = (g_lane == s.groups) | (g_lane == s.groups + 1)
    square = jnp.sum(jnp.where(squares, groups, 0.0), axis=1, keepdims=True)
    factor = lax.rsqrt(square / s.d + EPSILON)
    groups = groups * factor
    both = jnp.sum(partial[:, :, 0:wide].astype(F32), axis=0) * factor
    gate, up = both[:, : s.ff], both[:, s.ff :]
    hidden = (gate * (1.0 / (1.0 + jnp.exp(-gate))) * up).astype(BF16)
    output = matmul(hidden, down_w[...])
    logits = jnp.sum(partial[:, :, wide:tail].astype(F32), axis=0) * factor
    lane = lax.broadcasted_iota(jnp.int32, logits.shape, 1)
    chosen = jnp.sum(jnp.where(lane == expert, logits, 0.0), axis=1, keepdims=True)
    against = jnp.sum(jnp.where(lane == rival_id, logits, 0.0), axis=1, keepdims=True)
    own_group = lax.div(expert, s.experts // s.groups)
    g_own = jnp.sum(jnp.where(g_lane == own_group, groups, 0.0), axis=1, keepdims=True)
    shares = jnp.where(g_lane < s.groups, jnp.exp(groups - g_own), 0.0)
    share = 1.0 / jnp.sum(shares, axis=1, keepdims=True)
    weight = share * (1.0 / (1.0 + jnp.exp(against - chosen)))
    scaled = (output * weight).astype(BF16)

    merge_out[...] = matmul(own_there_t, scaled).astype(BF16)
    send(MERGE, merge_out, merge_in, partner)
    here = matmul(own_here_t, scaled)
    all_of(MERGE, merge_in).wait_recv()
    merged = (here + merge_in[...].astype(F32)).astype(BF16)
    combine_out[...] = merged.reshape(side // 2, 2, s.dq)
    for o in z_y:
        to = at(*o)
        send(COMBINE, combine_out.at[side_of(to[0], to[1])], combine_in.at[plane], to)
    combine_in[plane] = combine_out[side_of(z, y)]
    all_of(COMBINE, combine_in.at[pl.ds(0, len(z_y))]).wait_recv()
    moe_sum = jnp.sum(combine_in[...].astype(F32), axis=0)
    quarters[x] = (own_hidden[0:2] + moe_sum).astype(BF16)
    for o in x_only:
        send(QUARTERS, quarters.at[x], quarters.at[x], at(*o))
    all_of(QUARTERS, quarters.at[pl.ds(0, len(x_only))]).wait_recv()
    for j in range(s.X):
        quarter = quarters[j]
        for i in range(s.blocks):
            start = i * wide_block + j * chunk
            layer_out[:, start : start + chunk] = quarter[:, i * chunk : (i + 1) * chunk]

    all_of(PROJ_W, w_row.at[pl.ds(0, len(y_w) * s.rows), :]).wait_send()
    all_of(PROJ_T, normed_in.at[pl.ds(0, len(z_p))]).wait_send()
    all_of(RESIDUAL, residual_in.at[pl.ds(0, len(z_even))]).wait_send()
    all_of(OUT_W, out_w.at[pl.ds(0, len(out_from)), 0]).wait_send()
    all_of(OUT_PAIR, out_w.at[:, 0]).wait_send()
    all_of(PROJ_SUM, sums_out.at[pl.ds(0, len(z_p))]).wait_send()
    all_of(HEADS, heads.at[pl.ds(0, len(z_even))]).wait_send()
    all_of(HEAD_SUM, head_in.at[pl.ds(0, len(x_only))]).wait_send()
    all_of(GATHER, gathered.at[pl.ds(0, len(z_y))]).wait_send()
    all_of(PICKED, picked_out).wait_send()
    all_of(GATE_W, gate_w.at[:, :, pl.ds(0, 2 * len(x_only) * s.fh)]).wait_send()
    all_of(DOWN_W, down_w.at[pl.ds(0, len(x_only) * s.fh), :]).wait_send()
    all_of(GATE_SUM, partial.at[pl.ds(0, len(x_only))]).wait_send()
    all_of(MERGE, merge_out).wait_send()
    all_of(COMBINE, combine_in.at[pl.ds(0, len(z_y))]).wait_send()
    all_of(QUARTERS, quarters.at[pl.ds(0, len(x_only))]).wait_send()


def on_device(
    s,
    residual_in,
    gla_state,
    norm_gain,
    w_query,
    w_key,
    w_value,
    w_decay,
    decay_bias,
    head_gain,
    w_output,
    ffn_gain,
    router_group,
    router_expert,
    expert_ids,
    w_gate,
    w_up,
    w_down,
):
    old_state = gla_state[:, 0]
    side = s.tokens // 2
    vmem = pltpu.VMEM
    scratch = [
        vmem((2, s.d), BF16),
        vmem((s.d,), BF16),
        vmem((s.dkh,), F32),
        vmem((s.dvh,), BF16),
        vmem((s.d,), BF16),
        vmem((2, s.tokens), jnp.int32),
        vmem((2, s.dkh, s.dvh), F32),
        vmem((s.experts, s.dq), BF16),
        vmem((128, s.dq), BF16),
        vmem((2, s.rows, s.half), BF16),
        vmem((s.zb, s.half), BF16),
        vmem((s.Z, 2, s.zb), BF16),
        vmem((s.Z * 2 * s.C, 2, s.zb), BF16),
        vmem((2 * s.Y, s.C, s.rows, s.dvh), BF16),
        vmem((s.Z * 2 * s.C, 2, s.half), BF16),
        vmem((2, s.Z * 2, 2, s.half), BF16),
        vmem((s.blocks, 2, s.dvh), BF16),
        vmem((s.X, s.Z, s.chunk), BF16),
        vmem((s.X, s.Z, s.chunk), BF16),
        vmem((s.blocks, 2, s.chunk), BF16),
        vmem((s.Z * s.Y, s.Z, s.chunk), BF16),
        vmem((CAP, s.dq), BF16),
        vmem((CAP, s.dq), BF16),
        vmem((s.blocks, s.chunk, 2 * s.ff), BF16),
        vmem((s.ff, s.dq), BF16),
        vmem((s.X, CAP, 2 * s.ff + s.experts + 128), BF16),
        vmem((side, s.dq), BF16),
        vmem((side, s.dq), BF16),
        vmem((side // 2, 2, s.dq), BF16),
        vmem((side // 2, 2, s.dq), BF16),
        vmem((s.X, 2, s.dq), BF16),
        pltpu.SemaphoreType.DMA((32,)),
        pltpu.SemaphoreType.DMA((EXCHANGES,)),
        pltpu.SemaphoreType.DMA((EXCHANGES,)),
        pltpu.SemaphoreType.REGULAR,
    ]
    args = (
        residual_in,
        norm_gain,
        w_query,
        w_key,
        w_value,
        w_decay,
        decay_bias,
        old_state,
        head_gain,
        w_output.T,
        ffn_gain,
        router_group.T,
        router_expert,
        expert_ids.T,
        w_gate.reshape(s.blocks, s.X, s.chunk, s.fh),
        w_up.reshape(s.blocks, s.X, s.chunk, s.fh),
        w_down[0],
    )
    anywhere = pl.BlockSpec(memory_space=pl.ANY)
    layer_out, new_state = pl.pallas_call(
        functools.partial(layer_kernel, s),
        out_shape=(pltpu.VMEM((2, s.d), BF16), pltpu.VMEM((2, s.dkh, s.dvh), F32)),
        in_specs=[anywhere] * len(args),
        out_specs=(pl.BlockSpec(memory_space=vmem),) * 2,
        scratch_shapes=scratch,
        compiler_params=pltpu.CompilerParams(collective_id=0, has_side_effects=True),
        name="layer",
    )(*args)
    held = [pltpu.with_memory_space_constraint(a, vmem) for a in (layer_out, new_state)]
    layer_out, new_state = pl.pallas_call(
        store_kernel,
        out_shape=(
            jax.ShapeDtypeStruct((2, s.d), BF16),
            jax.ShapeDtypeStruct((2, s.dkh, s.dvh), F32),
        ),
        in_specs=[pl.BlockSpec(memory_space=vmem)] * 2,
        out_specs=(anywhere,) * 2,
        scratch_shapes=[pltpu.SemaphoreType.DMA((2,))],
        compiler_params=pltpu.CompilerParams(vmem_limit_bytes=1 << 20),
        name="store",
    )(*held)
    return layer_out, new_state[:, None]


def build(torus, residual, state, w_gate, router_group):
    Z, Y, C, X = (torus.shape[a] for a in AXES)
    tokens, d = residual
    experts, _, ff = w_gate
    dkh, dvh = state[2], state[3]
    s = types.SimpleNamespace(
        Z=Z,
        Y=Y,
        C=C,
        X=X,
        tokens=tokens,
        d=d,
        rows=d // (Z * Y * C),
        zb=d // Z,
        dq=d // X,
        blocks=Z // 2,
        chunk=2 * d // (Z * X),
        dkh=dkh,
        dvh=dvh,
        half=(3 * dkh + dvh) // 2,
        ff=ff,
        fh=ff // X,
        experts=experts,
        groups=router_group[1],
    )
    in_specs = (
        P(EP, None),
        P(EP, "x", None, None),
        P(),
        P(EP, "x"),
        P(EP, "x"),
        P(EP, "x"),
        P(EP, "x"),
        P("x"),
        P(),
        P("x", EP),
        P(),
        P(),
        P(),
        P(),
        P(EP, None, "x"),
        P(EP, None, "x"),
        P(EP, "x", None),
    )
    out_specs = (P(EP, None), P(EP, "x", None, None))
    return jax.shard_map(
        functools.partial(on_device, s),
        mesh=torus,
        in_specs=in_specs,
        out_specs=out_specs,
        check_vma=False,
    )


def solution(mesh):
    torus = Mesh(mesh.devices.reshape(8, 8, 2, mesh.shape["tp"]), AXES)

    def layer(*args):
        shapes = args[0].shape, args[1].shape, args[14].shape, args[11].shape
        return build(torus, *shapes)(*args)

    return layer
```

```python
import functools
import types

import jax
import jax.numpy as jnp
from jax import lax
from jax.experimental import pallas as pl
from jax.experimental.pallas import tpu as pltpu
from jax.sharding import Mesh
from jax.sharding import PartitionSpec as P

CAP = 16
EPSILON = 1e-06
GATE_SCALE = 16.0
AXES = ("z", "y", "c", "x")
EP = ("z", "y", "c")
MESH = pl.DeviceIdType.MESH
BF16 = jnp.bfloat16
F32 = jnp.float32

(
    PROJ_W,
    PROJ_T,
    RESIDUAL,
    OUT_W,
    OUT_Z,
    OUT_PAIR,
    OUT_PAIR_Z,
    PROJ_SUM,
    HEADS,
    HEAD_SUM,
    GATHER,
    PICKED,
    GATE_W,
    DOWN_W,
    GATE_SUM,
    MERGE,
    COMBINE,
    QUARTERS,
    EXCHANGES,
) = range(19)


def rounds(n, offset):
    return min(offset % n, -offset % n)


def rms_scale(values, gain):
    mean = jnp.mean(values * values, axis=-1, keepdims=True)
    return values * lax.rsqrt(mean + EPSILON) * gain


def matmul(a, b):
    return jnp.dot(a, b, preferred_element_type=F32)


def matmul_t(a, b):
    return lax.dot_general(a, b, (((1,), (1,)), ((), ())), preferred_element_type=F32)


def row_of(ref):
    return ref[...].astype(F32).reshape(1, ref.shape[0])


def store_kernel(layer, state, layer_out, state_out, sem):
    copies = [
        pltpu.make_async_copy(layer, layer_out, sem.at[0]),
        pltpu.make_async_copy(state, state_out, sem.at[1]),
    ]
    for copy in copies:
        copy.start()
    for copy in copies:
        copy.wait()


def layer_kernel(
    s,
    residual,
    norm_gain,
    w_query,
    w_key,
    w_value,
    w_decay,
    decay_bias,
    state,
    head_gain,
    w_output_t,
    ffn_gain,
    router_group_t,
    router_expert,
    ids_t,
    w_gate,
    w_up,
    w_down,
    layer_out,
    new_state,
    v_residual,
    v_norm_gain,
    v_bias,
    v_head_gain,
    v_ffn_gain,
    v_ids,
    v_state,
    v_router,
    v_group,
    w_own,
    w_row,
    normed_out,
    normed_in,
    out_w,
    sums_out,
    sums_in,
    heads,
    head_out,
    head_in,
    residual_in,
    gathered,
    picked_out,
    picked_in,
    gate_w,
    down_w,
    partial,
    merge_out,
    merge_in,
    combine_out,
    combine_in,
    quarters,
    load_sem,
    send_sem,
    recv_sem,
    plane_sem,
):
    z, y, c, x = (lax.axis_index(a) for a in AXES)
    other_c = 1 - c
    row = y * s.C + c
    plane = z * s.Y + y
    expert = plane * s.C + c
    half_w = s.half

    pair = lax.rem(y, 2)
    line = (z * 2 + pair) * s.C + c

    z_pair = lax.rem(z, 2)
    block = lax.div(z, 2)

    def at(dz=0, dy=0, dc=0, dx=0, across=0, across_z=0):
        return (
            z + 1 - 2 * z_pair if across_z else lax.rem(z + dz, s.Z) if dz else z,
            y + 1 - 2 * pair if across else lax.rem(y + dy, s.Y) if dy else y,
            lax.rem(c + dc, s.C) if dc else c,
            lax.rem(x + dx, s.X) if dx else x,
        )

    def ordered(offsets):
        def far(o):
            return -(rounds(s.Z, o[0]) + rounds(s.Y, o[1]) + rounds(s.X, o[3]) + sum(o[4:]))

        return sorted((o for o in offsets if any(o)), key=far)

    z_p = ordered((i, 0, k, 0, p) for i in range(s.Z) for k in range(s.C) for p in range(2))
    y_w = ordered((0, i, k, 0) for i in range(0, s.Y, 2) for k in range(s.C))
    y_c = ordered((0, i, k, 0) for i in range(s.Y) for k in range(s.C))
    z_only = ordered((i, 0, 0, 0) for i in range(s.Z))
    z_even = ordered((i, 0, 0, 0) for i in range(0, s.Z, 2))
    y_only = ordered((0, i, 0, 0) for i in range(s.Y))
    z_y = ordered((i, j, 0, 0) for i in range(s.Z) for j in range(s.Y))
    x_only = ordered((0, 0, 0, i) for i in range(s.X))
    partner = at(dc=1)

    def send(which, src, dst, device):
        pltpu.make_async_remote_copy(
            src_ref=src,
            dst_ref=dst,
            send_sem=send_sem.at[which],
            recv_sem=recv_sem.at[which],
            device_id=device,
            device_id_type=MESH,
        ).start()

    def all_of(which, ref):
        return pltpu.make_async_remote_copy(
            src_ref=ref,
            dst_ref=ref,
            send_sem=send_sem.at[which],
            recv_sem=recv_sem.at[which],
            device_id=partner,
            device_id_type=MESH,
        )

    def side_of(its_z, its_y):
        return (lax.rem(its_z, 2) * s.Y + its_y) * s.blocks + lax.div(its_z, 2)

    loads = []

    def load(src, dst):
        copy = pltpu.make_async_copy(src, dst, load_sem.at[len(loads)])
        loads.append(copy)
        copy.start()
        return copy

    k = s.dkh
    ld_weights = [
        load(w_query, w_own.at[0, :, pl.ds(0, k)]),
        load(w_key, w_own.at[0, :, pl.ds(k, k)]),
        load(w_decay.at[:, pl.ds(0, k // 2)], w_own.at[0, :, pl.ds(2 * k, k // 2)]),
        load(w_decay.at[:, pl.ds(k // 2, k // 2)], w_own.at[1, :, pl.ds(0, k // 2)]),
        load(w_value, w_own.at[1, :, pl.ds(k // 2, s.dvh)]),
    ]
    ld_residual = [load(residual, v_residual), load(norm_gain, v_norm_gain)]
    w_row[...] = jnp.zeros_like(w_row)
    barrier = pltpu.get_barrier_semaphore()
    greeted = ordered(y_c + [o for o in z_p if o[0]] + x_only)
    for o in greeted:
        pl.semaphore_signal(barrier, inc=1, device_id=at(*o), device_id_type=MESH)

    ld_ids = load(ids_t, v_ids)
    own_rows = pl.ds(pl.multiple_of(row * s.rows, s.rows), s.rows)
    chunk = s.chunk
    wide_block = s.X * chunk

    def chunk_of(i, j):
        return pl.ds(pl.multiple_of(i * wide_block + j * chunk, chunk), chunk)

    own_f = pl.ds(pl.multiple_of(x * s.fh, s.fh), s.fh)
    own_f2 = pl.ds(pl.multiple_of(s.ff + x * s.fh, s.fh), s.fh)
    ld_state = [load(decay_bias, v_bias), load(head_gain, v_head_gain), load(state, v_state)]
    v_group[...] = jnp.zeros_like(v_group)
    out_slot = z_pair * s.Y + y
    ld_out_w = [load(w_output_t, out_w.at[out_slot, c])]
    ld_ffn = [load(ffn_gain, v_ffn_gain)]
    ld_moe = [
        load(w_gate.at[:, x], gate_w.at[:, :, own_f]),
        load(w_up.at[:, x], gate_w.at[:, :, own_f2]),
    ]
    for i in range(s.blocks):
        cols = pl.ds(i * chunk, chunk)
        ld_moe.append(load(w_down.at[:, chunk_of(i, x)], down_w.at[own_f, cols]))
        ld_moe.append(load(router_expert.at[:, chunk_of(i, x)], v_router.at[:, cols]))
        ld_moe.append(
            load(router_group_t.at[:, chunk_of(i, x)], v_group.at[pl.ds(0, s.groups), cols])
        )

    for copy in ld_residual:
        copy.wait()
    normed = rms_scale(v_residual[...].astype(F32), row_of(v_norm_gain)).astype(BF16)
    for i in range(s.Z):
        normed_out[i] = normed[:, i * s.zb : (i + 1) * s.zb]
    for copy in ld_weights:
        copy.wait()

    pl.semaphore_wait(barrier, len(greeted))

    for o in z_p:
        to = at(*o)
        send(PROJ_T, normed_out.at[to[0]], normed_in.at[line], to)
    for o in y_w:
        to = at(*o)
        send(PROJ_W, w_own.at[to[2]], w_row.at[own_rows, :], to)
    for o in z_only:
        pl.semaphore_signal(plane_sem, inc=1, device_id=at(*o), device_id_type=MESH)
    for o in z_even:
        to = at(*o)
        theirs = chunk_of(lax.div(to[0], 2), x)
        send(RESIDUAL, v_residual.at[:, theirs], residual_in.at[block], to)
    for o in x_only:
        to = at(*o)
        send(GATE_W, w_gate.at[:, to[3]], gate_w.at[:, :, own_f], to)
        send(GATE_W, w_up.at[:, to[3]], gate_w.at[:, :, own_f2], to)
    for o in x_only:
        to = at(*o)
        for i in range(s.blocks):
            cols = pl.ds(i * chunk, chunk)
            send(DOWN_W, w_down.at[:, chunk_of(i, to[3])], down_w.at[own_f, cols], to)

    normed_in[line] = normed_out[z]
    residual_in[block] = v_residual[:, chunk_of(block, x)]
    w_row[own_rows, :] = w_own[c]
    combine_in[plane] = jnp.zeros((2, s.dq), BF16)

    for copy in ld_ffn:
        copy.wait()
    ld_ids.wait()
    tokens = s.tokens
    ids = v_ids[...]
    first, second = ids[0:1], ids[1:2]
    partner_expert = plane * s.C + other_c
    own_named = ((first == expert) | (second == expert)).astype(F32)
    par_named = ((first == partner_expert) | (second == partner_expert)).astype(F32)
    named = jnp.concatenate([own_named, par_named, jnp.zeros((6, tokens), F32)], axis=0)
    t_row = lax.broadcasted_iota(jnp.int32, (tokens, tokens), 0)
    t_col = lax.broadcasted_iota(jnp.int32, (tokens, tokens), 1)
    upto = (t_row <= t_col).astype(BF16)
    code = named * matmul(named.astype(BF16), upto)
    slot_full = lax.broadcasted_iota(jnp.int32, (CAP, tokens), 0).astype(F32) + 1.0
    rival = jnp.where(first == expert, second, first).astype(F32)
    own_full = jnp.where(slot_full == code[0:1], 1.0, 0.0)
    rival_id = jnp.sum(own_full * rival, axis=1, keepdims=True).astype(jnp.int32)
    side = tokens // 2
    p_row = lax.broadcasted_iota(jnp.int32, (tokens, side), 0)
    p_col = lax.broadcasted_iota(jnp.int32, (tokens, side), 1)
    per_z = s.Y * s.Z
    p_y = lax.div(lax.rem(p_col, per_z), s.Z)
    p_z = 2 * lax.div(lax.rem(p_col, s.Z), 2) + lax.div(p_col, per_z)
    p_tok = (p_z * s.Y + p_y) * 2 * s.C + lax.rem(p_col, 2)
    slot_side = lax.broadcasted_iota(jnp.int32, (CAP, side), 0).astype(F32) + 1.0
    code_c = matmul(code.astype(BF16), (p_row == p_tok + 2 * c).astype(BF16))
    code_o = matmul(code.astype(BF16), (p_row == p_tok + 2 * other_c).astype(BF16))
    own_here = (slot_side == code_c[0:1]).astype(F32)
    par_here = (slot_side == code_c[1:2]).astype(F32)
    own_there = (slot_side == code_o[0:1]).astype(F32)
    o_row = lax.broadcasted_iota(jnp.int32, (8, side), 0)
    o_col = lax.broadcasted_iota(jnp.int32, (8, side), 1)
    own_pick = (o_col == 2 * side_of(z, y) + o_row) & (o_row < 2)
    gains = row_of(v_ffn_gain)
    gain = jnp.zeros((1, s.dq), F32)
    for j in range(s.X):
        starts = [i * wide_block + j * chunk for i in range(s.blocks)]
        piece = jnp.concatenate([gains[:, a : a + chunk] for a in starts], axis=1)
        gain = gain + jnp.where(x == j, piece, 0.0)
    own_here_t = own_here.T.astype(BF16)
    own_there_t = own_there.T.astype(BF16)

    all_of(PROJ_T, normed_in.at[pl.ds(0, len(z_p))]).wait_recv()
    ld_out_w[0].wait()
    for o in y_only:
        send(OUT_W, out_w.at[out_slot, c], out_w.at[out_slot, c], at(*o))
    all_of(PROJ_W, w_row.at[pl.ds(0, len(y_w) * s.rows), :]).wait_recv()
    lines = s.Z * 2 * s.C
    sums = matmul(normed_in[...].reshape(2 * lines, s.zb), w_row[...])
    sums_out[...] = sums.astype(BF16).reshape(lines, 2, half_w)
    for o in z_p:
        to = at(*o)
        to_line = (to[0] * 2 + lax.rem(to[1], 2)) * s.C + to[2]
        send(PROJ_SUM, sums_out.at[to_line], sums_in.at[c, z * 2 + pair], to)
    sums_in[c, z * 2 + pair] = sums_out[line]
    here = pl.ds(pl.multiple_of(z_pair * s.Y, s.Y), s.Y)
    there = pl.ds(pl.multiple_of((1 - z_pair) * s.Y, s.Y), s.Y)
    all_of(OUT_W, out_w.at[pl.ds(0, len(y_only)), 0]).wait_recv()
    send(OUT_Z, out_w.at[here].at[:, c], out_w.at[here].at[:, c], at(across_z=1))
    send(OUT_PAIR, out_w.at[here].at[:, c], out_w.at[here].at[:, c], partner)

    for copy in ld_state:
        copy.wait()
    all_of(PROJ_SUM, sums_out.at[pl.ds(0, len(z_p))]).wait_recv()
    low = jnp.sum(sums_in[0].astype(F32), axis=0)
    high = jnp.sum(sums_in[1].astype(F32), axis=0)
    query = low[:, :k].astype(BF16).astype(F32) * k ** (-0.5)
    key = low[:, k : 2 * k].astype(BF16).astype(F32)
    decay = jnp.concatenate([low[:, 2 * k :], high[:, : k // 2]], axis=1) + row_of(v_bias)
    value = high[:, k // 2 :].astype(BF16).astype(F32)
    log_decay = jnp.minimum(decay, 0.0) - jnp.log1p(jnp.exp(-jnp.abs(decay)))
    alpha = jnp.exp(log_decay / GATE_SCALE)
    factors = jnp.concatenate([query * alpha, alpha, key, jnp.zeros((2, k), F32)], axis=0).T
    read_out = jnp.concatenate(
        [
            jnp.sum(factors[:, 0:1] * v_state[0], axis=0, keepdims=True),
            jnp.sum(factors[:, 1:2] * v_state[1], axis=0, keepdims=True),
        ],
        axis=0,
    )
    read_out = read_out + jnp.sum(query * key, axis=1, keepdims=True) * value
    heads[block] = rms_scale(read_out, row_of(v_head_gain)).astype(BF16)
    for o in z_even:
        send(HEADS, heads.at[block], heads.at[block], at(*o))
    all_of(OUT_Z, out_w.at[pl.ds(0, s.Y), 0]).wait_recv()
    send(OUT_PAIR_Z, out_w.at[there].at[:, c], out_w.at[there].at[:, c], partner)
    for i in range(2):
        carried = factors[:, 2 + i : 3 + i] * v_state[i]
        new_state[i] = carried + factors[:, 4 + i : 5 + i] * value[i : i + 1]

    all_of(RESIDUAL, residual_in.at[pl.ds(0, len(z_even))]).wait_recv()
    all_of(OUT_PAIR, out_w.at[pl.ds(0, s.Y), 0]).wait_recv()
    all_of(OUT_PAIR_Z, out_w.at[pl.ds(0, s.Y), 0]).wait_recv()
    all_of(HEADS, heads.at[pl.ds(0, len(z_even))]).wait_recv()
    part = matmul_t(heads[...].reshape(s.Z, s.dvh), out_w[...].reshape(wide_block, s.dvh))
    part = part.astype(BF16)
    for j in range(s.X):
        head_out[j] = part[:, j * chunk : (j + 1) * chunk]
    for o in x_only:
        to = at(*o)
        send(HEAD_SUM, head_out.at[to[3]], head_in.at[x], to)
    head_in[x] = head_out[x]
    pl.semaphore_wait(plane_sem, len(z_only))
    all_of(HEAD_SUM, head_in.at[pl.ds(0, len(x_only))]).wait_recv()
    attention = head_in[0].astype(F32)
    for j in range(1, s.X):
        attention = attention + head_in[j].astype(F32)
    residual_rows = residual_in[...].reshape(s.Z, chunk).astype(F32)
    gathered[plane] = (residual_rows + attention).astype(BF16)

    for o in z_y:
        send(GATHER, gathered.at[plane], gathered.at[plane], at(*o))
    for copy in ld_moe:
        copy.wait()
    all_of(GATHER, gathered.at[pl.ds(0, len(z_y))]).wait_recv()
    rows = jnp.concatenate(
        [
            gathered[pl.ds(2 * s.Y * i, 2 * s.Y)].reshape(side, chunk)
            for i in range(s.blocks)
        ],
        axis=1,
    )
    picked_out[...] = matmul(par_here.astype(BF16), rows).astype(BF16)
    send(PICKED, picked_out, picked_in, partner)
    picked = matmul(own_here.astype(BF16), rows)
    own_hidden = matmul(own_pick.astype(BF16), rows)
    all_of(GATE_W, gate_w.at[:, :, pl.ds(0, 2 * len(x_only) * s.fh)]).wait_recv()
    all_of(PICKED, picked_in).wait_recv()
    picked = picked + picked_in[...].astype(F32)
    square = jnp.sum(picked * picked, axis=1, keepdims=True)
    picked = (picked * gain).astype(BF16)
    wide = 2 * s.ff
    partial[x, :, 0:wide] = matmul(picked, gate_w[...].reshape(s.dq, wide)).astype(BF16)
    logits = matmul_t(picked, v_router[...])
    groups = matmul_t(picked, v_group[...])
    lane = lax.broadcasted_iota(jnp.int32, logits.shape, 1)
    ahead = jnp.where(lane == expert, logits, jnp.where(lane == rival_id, -logits, 0.0))
    ahead = jnp.sum(ahead, axis=1, keepdims=True)
    ahead_high = ahead.astype(BF16).astype(F32)
    g_lane = lax.broadcasted_iota(jnp.int32, groups.shape, 1)
    high = square.astype(BF16).astype(F32)
    groups = jnp.where(g_lane == s.groups, high, groups)
    groups = jnp.where(g_lane == s.groups + 1, square - high, groups)
    groups = jnp.where(g_lane == s.groups + 2, ahead_high, groups)
    groups = jnp.where(g_lane == s.groups + 3, ahead - ahead_high, groups)
    partial[x, :, wide : wide + 128] = groups.astype(BF16)
    for o in x_only:
        send(GATE_SUM, partial.at[x], partial.at[x], at(*o))
    all_of(DOWN_W, down_w.at[pl.ds(0, len(x_only) * s.fh), :]).wait_recv()
    all_of(GATE_SUM, partial.at[pl.ds(0, len(x_only))]).wait_recv()
    groups = jnp.sum(partial[:, :, wide : wide + 128].astype(F32), axis=0)
    squares = (g_lane == s.groups) | (g_lane == s.groups + 1)
    square = jnp.sum(jnp.where(squares, groups, 0.0), axis=1, keepdims=True)
    factor = lax.rsqrt(square / s.d + EPSILON)
    groups = groups * factor
    both = jnp.sum(partial[:, :, 0:wide].astype(F32), axis=0) * factor
    gate, up = both[:, : s.ff], both[:, s.ff :]
    hidden = (gate * (1.0 / (1.0 + jnp.exp(-gate))) * up).astype(BF16)
    output = matmul(hidden, down_w[...])
    leads = (g_lane == s.groups + 2) | (g_lane == s.groups + 3)
    ahead = jnp.sum(jnp.where(leads, groups, 0.0), axis=1, keepdims=True)
    own_group = lax.div(expert, s.experts // s.groups)
    g_own = jnp.sum(jnp.where(g_lane == own_group, groups, 0.0), axis=1, keepdims=True)
    shares = jnp.where(g_lane < s.groups, jnp.exp(groups - g_own), 0.0)
    share = 1.0 / jnp.sum(shares, axis=1, keepdims=True)
    weight = share * (1.0 / (1.0 + jnp.exp(-ahead)))
    scaled = (output * weight).astype(BF16)

    merge_out[...] = matmul(own_there_t, scaled).astype(BF16)
    send(MERGE, merge_out, merge_in, partner)
    here = matmul(own_here_t, scaled)
    all_of(MERGE, merge_in).wait_recv()
    merged = (here + merge_in[...].astype(F32)).astype(BF16)
    combine_out[...] = merged
    for o in z_y:
        to = at(*o)
        theirs = pl.ds(pl.multiple_of(2 * side_of(to[0], to[1]), 2), 2)
        send(COMBINE, combine_out.at[theirs, :], combine_in.at[plane], to)
    own_moe = matmul(own_pick.astype(BF16), merged)
    all_of(COMBINE, combine_in.at[pl.ds(0, len(z_y))]).wait_recv()
    moe_sum = own_moe[0:2] + jnp.sum(combine_in[...].astype(F32), axis=0)
    quarters[x] = (own_hidden[0:2] + moe_sum).astype(BF16)
    for o in x_only:
        send(QUARTERS, quarters.at[x], quarters.at[x], at(*o))
    all_of(PROJ_W, w_row.at[pl.ds(0, len(y_w) * s.rows), :]).wait_send()
    all_of(PROJ_T, normed_in.at[pl.ds(0, len(z_p))]).wait_send()
    all_of(RESIDUAL, residual_in.at[pl.ds(0, len(z_even))]).wait_send()
    all_of(OUT_W, out_w.at[pl.ds(0, len(y_only)), 0]).wait_send()
    all_of(OUT_Z, out_w.at[pl.ds(0, s.Y), 0]).wait_send()
    all_of(OUT_PAIR, out_w.at[pl.ds(0, s.Y), 0]).wait_send()
    all_of(OUT_PAIR_Z, out_w.at[pl.ds(0, s.Y), 0]).wait_send()
    all_of(PROJ_SUM, sums_out.at[pl.ds(0, len(z_p))]).wait_send()
    all_of(HEADS, heads.at[pl.ds(0, len(z_even))]).wait_send()
    all_of(HEAD_SUM, head_in.at[pl.ds(0, len(x_only))]).wait_send()
    all_of(GATHER, gathered.at[pl.ds(0, len(z_y))]).wait_send()
    all_of(PICKED, picked_out).wait_send()
    all_of(GATE_W, gate_w.at[:, :, pl.ds(0, 2 * len(x_only) * s.fh)]).wait_send()
    all_of(DOWN_W, down_w.at[pl.ds(0, len(x_only) * s.fh), :]).wait_send()
    all_of(GATE_SUM, partial.at[pl.ds(0, len(x_only))]).wait_send()
    all_of(MERGE, merge_out).wait_send()
    all_of(COMBINE, combine_in.at[pl.ds(0, len(z_y))]).wait_send()
    all_of(QUARTERS, quarters.at[pl.ds(0, len(x_only))]).wait_recv()
    for j in range(s.X):
        quarter = quarters[j]
        for i in range(s.blocks):
            start = i * wide_block + j * chunk
            layer_out[:, start : start + chunk] = quarter[:, i * chunk : (i + 1) * chunk]
    all_of(QUARTERS, quarters.at[pl.ds(0, len(x_only))]).wait_send()


def on_device(
    s,
    residual_in,
    gla_state,
    norm_gain,
    w_query,
    w_key,
    w_value,
    w_decay,
    decay_bias,
    head_gain,
    w_output,
    ffn_gain,
    router_group,
    router_expert,
    expert_ids,
    w_gate,
    w_up,
    w_down,
):
    old_state = gla_state[:, 0]
    side = s.tokens // 2
    vmem = pltpu.VMEM
    scratch = [
        vmem((2, s.d), BF16),
        vmem((s.d,), BF16),
        vmem((s.dkh,), F32),
        vmem((s.dvh,), BF16),
        vmem((s.d,), BF16),
        vmem((2, s.tokens), jnp.int32),
        vmem((2, s.dkh, s.dvh), F32),
        vmem((s.experts, s.dq), BF16),
        vmem((128, s.dq), BF16),
        vmem((2, s.rows, s.half), BF16),
        vmem((s.zb, s.half), BF16),
        vmem((s.Z, 2, s.zb), BF16),
        vmem((s.Z * 2 * s.C, 2, s.zb), BF16),
        vmem((2 * s.Y, s.C, s.rows, s.dvh), BF16),
        vmem((s.Z * 2 * s.C, 2, s.half), BF16),
        vmem((2, s.Z * 2, 2, s.half), BF16),
        vmem((s.blocks, 2, s.dvh), BF16),
        vmem((s.X, s.Z, s.chunk), BF16),
        vmem((s.X, s.Z, s.chunk), BF16),
        vmem((s.blocks, 2, s.chunk), BF16),
        vmem((s.Z * s.Y, s.Z, s.chunk), BF16),
        vmem((CAP, s.dq), BF16),
        vmem((CAP, s.dq), BF16),
        vmem((s.blocks, s.chunk, 2 * s.ff), BF16),
        vmem((s.ff, s.dq), BF16),
        vmem((s.X, CAP, 2 * s.ff + 128), BF16),
        vmem((side, s.dq), BF16),
        vmem((side, s.dq), BF16),
        vmem((side, s.dq), BF16),
        vmem((side // 2, 2, s.dq), BF16),
        vmem((s.X, 2, s.dq), BF16),
        pltpu.SemaphoreType.DMA((32,)),
        pltpu.SemaphoreType.DMA((EXCHANGES,)),
        pltpu.SemaphoreType.DMA((EXCHANGES,)),
        pltpu.SemaphoreType.REGULAR,
    ]
    args = (
        residual_in,
        norm_gain,
        w_query,
        w_key,
        w_value,
        w_decay,
        decay_bias,
        old_state,
        head_gain,
        w_output.T,
        ffn_gain,
        router_group.T,
        router_expert,
        expert_ids.T,
        w_gate.reshape(s.blocks, s.X, s.chunk, s.fh),
        w_up.reshape(s.blocks, s.X, s.chunk, s.fh),
        w_down[0],
    )
    anywhere = pl.BlockSpec(memory_space=pl.ANY)
    layer_out, new_state = pl.pallas_call(
        functools.partial(layer_kernel, s),
        out_shape=(pltpu.VMEM((2, s.d), BF16), pltpu.VMEM((2, s.dkh, s.dvh), F32)),
        in_specs=[anywhere] * len(args),
        out_specs=(pl.BlockSpec(memory_space=vmem),) * 2,
        scratch_shapes=scratch,
        compiler_params=pltpu.CompilerParams(collective_id=0, has_side_effects=True),
        name="layer",
    )(*args)
    held = [pltpu.with_memory_space_constraint(a, vmem) for a in (layer_out, new_state)]
    layer_out, new_state = pl.pallas_call(
        store_kernel,
        out_shape=(
            jax.ShapeDtypeStruct((2, s.d), BF16),
            jax.ShapeDtypeStruct((2, s.dkh, s.dvh), F32),
        ),
        in_specs=[pl.BlockSpec(memory_space=vmem)] * 2,
        out_specs=(anywhere,) * 2,
        scratch_shapes=[pltpu.SemaphoreType.DMA((2,))],
        compiler_params=pltpu.CompilerParams(vmem_limit_bytes=1 << 20),
        name="store",
    )(*held)
    return layer_out, new_state[:, None]


def build(torus, residual, state, w_gate, router_group):
    Z, Y, C, X = (torus.shape[a] for a in AXES)
    tokens, d = residual
    experts, _, ff = w_gate
    dkh, dvh = state[2], state[3]
    s = types.SimpleNamespace(
        Z=Z,
        Y=Y,
        C=C,
        X=X,
        tokens=tokens,
        d=d,
        rows=d // (Z * Y * C),
        zb=d // Z,
        dq=d // X,
        blocks=Z // 2,
        chunk=2 * d // (Z * X),
        dkh=dkh,
        dvh=dvh,
        half=(3 * dkh + dvh) // 2,
        ff=ff,
        fh=ff // X,
        experts=experts,
        groups=router_group[1],
    )
    in_specs = (
        P(EP, None),
        P(EP, "x", None, None),
        P(),
        P(EP, "x"),
        P(EP, "x"),
        P(EP, "x"),
        P(EP, "x"),
        P("x"),
        P(),
        P("x", EP),
        P(),
        P(),
        P(),
        P(),
        P(EP, None, "x"),
        P(EP, None, "x"),
        P(EP, "x", None),
    )
    out_specs = (P(EP, None), P(EP, "x", None, None))
    return jax.shard_map(
        functools.partial(on_device, s),
        mesh=torus,
        in_specs=in_specs,
        out_specs=out_specs,
        check_vma=False,
    )


def solution(mesh):
    torus = Mesh(mesh.devices.reshape(8, 8, 2, mesh.shape["tp"]), AXES)

    def layer(*args):
        shapes = args[0].shape, args[1].shape, args[14].shape, args[11].shape
        return build(torus, *shapes)(*args)

    return layer
```
